32 devices in a mesh: ep: 8 (over z, core), tp: 4 (over y, x).
Axes of the slice: x: 2, y: 2, z: 4, core: 2. Of those that a mesh axis runs over, the one named last changes fastest.
Arguments:
- query_input: bfloat16 [4096, 2048], P('ep', 'tp'), may hold values from -6 to 6
- key_input: bfloat16 [4096, 1024], P('ep', 'tp'), may hold values from -6 to 6
- value_input: bfloat16 [4096, 1024], P('ep', 'tp'), may hold values from -64 to 64
- query_gain: float32 [64], replicated, may hold values from 0.5 to 6
- key_gain: float32 [64], replicated, may hold values from 0.5 to 6
- mixer_out: bfloat16 [2048, 4096], P(None, 'tp'), may hold values from -0.125 to 0.125
- moe_input: bfloat16 [2048, 4096], P('ep'), may hold values from -6 to 6
- moe_gain: float32 [4096], replicated, may hold values from 0.1 to 1.9
- routes: int32 [2048, 2], P('ep'), may hold values from 0 to 7, all different within a row; in each aligned block of 256 rows (0 to 255, 256 to 511, ...) at most 96 rows name the same one
- route_weight: float32 [2048, 2], P('ep'), may hold values from 0.1 to 1
- expert_gate: bfloat16 [8, 4096, 1024], P('ep', None, 'tp'), may hold values from -0.09375 to 0.09375
- expert_up: bfloat16 [8, 4096, 1024], P('ep', None, 'tp'), may hold values from -0.09375 to 0.09375
- expert_down: bfloat16 [8, 1024, 4096], P('ep', None, 'tp'), may hold values from -0.1875 to 0.1875
Outputs:
- attn_mixed: bfloat16 [4096, 4096], P('ep', 'tp')
- moe_out: bfloat16 [2048, 4096], P('ep', 'tp')
The draws below stay inside these ranges and needn't reach their ends.
Inputs may be any that keep to these rules, and one draw needn't show every extreme that they name: `routes`: each row names 2 different experts. In the rows of one index of ep (aligned blocks of 256 rows) no expert is named by more than 96 rows, and in every draw some block has an expert named by exactly 96 rows.
All inputs are finite; a program needn't handle non-finite values.
Results may differ from the reference program's by a relative error of at most 0.0095.
The reference program's roundings to bfloat16 on the way count: a program that leaves them out, or rounds other values in their place, can miss the bound.
Values may be sent and summed in bfloat16 or wider, within the bound.
A program may use at most 64 MiB of HBM per device.

```python
import math
import jax
import jax.numpy as jnp
import numpy as np
from jax import lax

D = 4096
HEADS = 32
KV_HEADS = 16
HEAD_DIM = 64
FF = 1024
GRID_W = 64
TOP_K = 2
MOE_TOK = 256
SEQ_LEN = 4096
MOE_TOKENS = 2048
EXPERTS = 8
CAP = 96
N_EP = 8


def draw_query_input(key, part):
    column_count = HEADS * HEAD_DIM
    samples = jnp.clip(jax.random.normal(jax.random.fold_in(key, 101), (SEQ_LEN, column_count), jnp.float32), -6.0, 6.0)
    return samples.astype(jnp.bfloat16)


def draw_key_input(key, part):
    column_count = KV_HEADS * HEAD_DIM
    samples = jnp.clip(jax.random.normal(jax.random.fold_in(key, 202), (SEQ_LEN, column_count), jnp.float32), -6.0, 6.0)
    return samples.astype(jnp.bfloat16)


def draw_query_gain(key, part):
    spread = jax.random.uniform(jax.random.fold_in(key, 303), (HEAD_DIM,), jnp.float32, jnp.log(0.5), jnp.log(2.0))
    gains = jnp.exp(spread)
    return gains.astype(jnp.float32)


def draw_key_gain(key, part):
    spread = jax.random.uniform(jax.random.fold_in(key, 404), (HEAD_DIM,), jnp.float32, jnp.log(0.5), jnp.log(2.0))
    gains = jnp.exp(spread)
    return gains.astype(jnp.float32)


def block_levels(key, shape, pieces, least, high):
    def one(axis_at, blocks):
        heights = jax.random.uniform(jax.random.fold_in(jax.random.fold_in(key, 6), axis_at), (blocks,), jnp.float32, least / len(pieces), high / len(pieces))
        return jnp.repeat(jnp.exp(heights), shape[axis_at] // blocks).reshape((-1,) + (1,) * (len(shape) - axis_at - 1))

    factor_of = one(*pieces[0])
    for cut in pieces[1:]:
        factor_of = factor_of * one(*cut)
    return factor_of


def routed_block(stream_key, own, number, rows, amount, top, bound, skew):
    order = jax.random.permutation(stream_key, amount)
    packed, common = portions_of(amount, rows * top, bound, skew, True), portions_of(amount, rows * top, bound, skew, False)
    places = jnp.arange(amount)

    def named(tallies, rotation):
        used = int((tallies > 0).sum())
        fixed = max(1, used // 4)
        moved = fixed + (places - fixed + rotation * (used - fixed)) % max(1, amount - fixed)
        return jnp.zeros((amount,), jnp.int32).at[order[jnp.where(places < fixed, places, moved)]].set(jnp.asarray(tallies, jnp.int32))

    tallies = jnp.where(number % 4 == 0, named(packed, number // 4), named(common, number - number // 4 - 1))
    mixed = jax.random.permutation(jax.random.fold_in(own, 3), amount)
    source_of, sink = mixed[0:amount // 2 * 2:2], mixed[1:amount // 2 * 2:2]
    slack = jnp.minimum(tallies[source_of] - 1, bound - tallies[sink]) // 2
    slack = jnp.where((source_of == order[0]) | (sink == order[0]) | (tallies[sink] == 0), 0, jnp.maximum(slack, 0))
    moved = jax.random.randint(jax.random.fold_in(own, 4), (amount // 2,), 0, 1 << 20) % (slack + 1)
    tallies = tallies.at[source_of].add(-moved).at[sink].add(moved)
    labels = jnp.searchsorted(jnp.cumsum(tallies), jnp.arange(rows * top), side="right").astype(jnp.int32)
    listing = labels.reshape(top, rows).T
    listing = listing[jax.random.permutation(jax.random.fold_in(own, 1), rows)]
    rotation = jax.random.randint(jax.random.fold_in(own, 2), (rows, 1), 0, top)
    return jnp.take_along_axis(listing, (jnp.arange(top)[None, :] + rotation) % top, axis=1)


def portions_of(amount, total, reach, skew, full):
    weights = [(1 << 20) // math.isqrt(rank ** skew) + 1 for rank in range(1, amount + 1)]
    largest = reach if full else min(reach, max(-(-total // amount), total * weights[0] // sum(weights)))
    least = 1 if total - largest >= amount - 1 else 0
    counts, rest = [largest] + [least] * (amount - 1), total - largest - least * (amount - 1)
    while rest > 0:
        movable = [i for i in range(1, amount) if counts[i] < largest] or [i for i in range(1, amount) if counts[i] < reach]
        pool, left = sum([weights[i] for i in movable]), rest
        for i in movable:
            addition = min(reach - counts[i], max(1, left * weights[i] // pool), rest)
            counts[i] = counts[i] + addition
            rest = rest - addition
    return np.array(counts)


def scatter_about(stream_key, dims, scale, bound, cuts=(), held_as=jnp.bfloat16):
    result = jax.random.normal(stream_key, dims, jnp.float32) * scale
    if len(cuts) > 0:
        result = block_levels(stream_key, dims, cuts, -0.22, 0.18) * result
    return jnp.clip(result, min=-bound, max=bound).astype(held_as)


def setup_inputs(seed: int = 0) -> dict:
    streams_of = jax.random.split(jax.random.key(seed), 14)
    query_input = draw_query_input(jax.random.fold_in(streams_of[13], 71), 0)
    key_input = draw_key_input(jax.random.fold_in(streams_of[13], 71), 0)
    value_input = jnp.clip(jax.random.uniform(streams_of[2], (SEQ_LEN, KV_HEADS * HEAD_DIM), jnp.float32, -64.0, 64.0) * block_levels(streams_of[2], (SEQ_LEN, KV_HEADS * HEAD_DIM), ((0, 8), (1, 4)), -0.4, 0.0), -64.0, 64.0).astype(jnp.bfloat16)
    query_gain = draw_query_gain(jax.random.fold_in(streams_of[13], 71), 0)
    key_gain = draw_key_gain(jax.random.fold_in(streams_of[13], 71), 0)
    mixer_out = scatter_about(streams_of[5], (HEADS * HEAD_DIM, D), (HEADS * HEAD_DIM) ** -0.5, 0.125, ((1, 4),))
    moe_input = scatter_about(streams_of[6], (MOE_TOKENS, D), 1.0, 6.0, ((0, 8),))
    moe_gain = jnp.clip(1.0 + 0.18 * jax.random.normal(streams_of[7], (D,), jnp.float32), 0.1, 1.9)
    routes_keys = jax.random.split(jax.random.fold_in(streams_of[8], 1), MOE_TOKENS // MOE_TOK)
    routes_turns = jax.random.permutation(jax.random.fold_in(streams_of[8], 3), MOE_TOKENS // MOE_TOK)
    routes = jax.vmap(lambda own, number: routed_block(jax.random.fold_in(streams_of[8], 2), own, number, MOE_TOK, EXPERTS, TOP_K, CAP, 1))(routes_keys, routes_turns).reshape((MOE_TOKENS, TOP_K))
    route_weight = jnp.clip(jnp.exp(math.log(1.0) - 2.3025851 * jax.random.uniform(streams_of[9], (MOE_TOKENS, TOP_K), jnp.float32) ** block_levels(streams_of[9], (MOE_TOKENS, TOP_K), ((0, 8),), -0.2, 0.2)), 0.1, 1.0)
    expert_gate = scatter_about(streams_of[10], (EXPERTS, D, FF), D ** -0.5, 0.09375, ((0, 8), (2, 4)))
    expert_up = scatter_about(streams_of[11], (EXPERTS, D, FF), D ** -0.5, 0.09375, ((0, 8), (2, 4)))
    expert_down = scatter_about(streams_of[12], (EXPERTS, FF, D), FF ** -0.5, 0.1875, ((0, 8), (2, 4)))
    return {"query_input": query_input, "key_input": key_input, "value_input": value_input, "query_gain": query_gain, "key_gain": key_gain, "mixer_out": mixer_out, "moe_input": moe_input, "moe_gain": moe_gain, "routes": routes, "route_weight": route_weight, "expert_gate": expert_gate, "expert_up": expert_up, "expert_down": expert_down}


epsilon = 1e-06
base_theta = 10000.0

def rope_tables(positions, head_width):
    quarter = head_width // 4
    inverse = base_theta ** (-jnp.arange(quarter, dtype=jnp.float32) / quarter)
    grid_row = (positions // GRID_W).astype(jnp.float32)
    grid_col = (positions % GRID_W).astype(jnp.float32)
    angles = jnp.concatenate([grid_row[:, None] * inverse[None, :], grid_col[:, None] * inverse[None, :]], axis=1)
    return (jnp.cos(angles), jnp.sin(angles))

def head_norm(heads_in, gain):
    return heads_in * lax.rsqrt(lax.optimization_barrier(jnp.mean(heads_in * heads_in, axis=-1, keepdims=True)) + epsilon) * gain

def rotate(heads_in, cosine, sine_table):
    half_width = heads_in.shape[-1] // 2
    first_half = heads_in[..., :half_width]
    second_half = heads_in[..., half_width:]
    cos_rows = cosine[:, None, :]
    sin_rows = sine_table[:, None, :]
    return jnp.concatenate([first_half * cos_rows - second_half * sin_rows, first_half * sin_rows + second_half * cos_rows], axis=-1)

def slot_places(route_block, expert_count, capacity):
    flat_routes = route_block.reshape(-1)
    one_hot = (flat_routes[:, None] == jnp.arange(expert_count, dtype=jnp.int32)[None, :]).astype(jnp.int32)
    earlier = jnp.cumsum(one_hot, axis=0) - one_hot
    return (flat_routes * capacity + lax.optimization_barrier(jnp.sum(earlier * one_hot, axis=1))).astype(jnp.int32)

def fill_sources(places, token_count, top_count, slot_total):
    source_rows = jnp.full((slot_total,), token_count, jnp.int32)
    pair_rows = (jnp.arange(token_count * top_count, dtype=jnp.int32) // top_count).astype(jnp.int32)
    return source_rows.at[places].set(pair_rows)

def attend(query_rot, key_rot, value_input):
    seq_len = query_rot.shape[0]
    group_size = HEADS // KV_HEADS
    block_len = math.gcd(seq_len, 128)
    key_all = key_rot.astype(jnp.float32)
    value_all = value_input.astype(jnp.float32).reshape(seq_len, KV_HEADS, HEAD_DIM)
    blocks = query_rot.astype(jnp.float32).reshape(seq_len // block_len, block_len, KV_HEADS, group_size, HEAD_DIM)
    score_scale = HEAD_DIM ** (-0.5)

    def one_block(query_block):
        scores = jnp.einsum('qkgd,skd->kgqs', query_block, key_all) * score_scale
        largest = lax.optimization_barrier(jnp.max(scores, axis=-1, keepdims=True))
        weights = jnp.exp(scores - largest)
        denominator = lax.optimization_barrier(jnp.sum(weights, axis=-1))
        rounded = lax.optimization_barrier(weights.astype(jnp.bfloat16)).astype(jnp.float32)
        numerator = jnp.einsum('kgqs,skd->qkgd', rounded, value_all)
        return numerator / jnp.transpose(denominator, (2, 0, 1))[..., None]
    attended = lax.map(one_block, blocks)
    return attended.reshape(seq_len, HEADS * HEAD_DIM).astype(jnp.bfloat16)

def experts_layer(moe_input, moe_gain, routes, route_weight, expert_gate, expert_up, expert_down):
    features = moe_input.astype(jnp.float32)
    normed = (features * lax.rsqrt(lax.optimization_barrier(jnp.mean(features * features, axis=-1, keepdims=True)) + epsilon) * moe_gain).astype(jnp.bfloat16)
    blocks = normed.reshape(N_EP, MOE_TOK, D)
    places = jax.vmap(lambda route_block: slot_places(route_block, EXPERTS, CAP))(routes.reshape(N_EP, MOE_TOK, TOP_K))
    sources = jax.vmap(lambda place_row: fill_sources(place_row, MOE_TOK, TOP_K, EXPERTS * CAP))(places)
    padded = jnp.concatenate([blocks, jnp.zeros((N_EP, 1, D), jnp.bfloat16)], axis=1)
    gathered = jax.vmap(lambda padded_block, source_row: padded_block[source_row])(padded, sources)
    per_expert = gathered.reshape(N_EP, EXPERTS, CAP, D).transpose(1, 0, 2, 3).reshape(EXPERTS, N_EP * CAP, D)

    def one_expert(operands):
        expert_rows, gate_matrix, up_matrix, down_matrix = operands
        gate_hidden = jnp.dot(expert_rows, gate_matrix, preferred_element_type=jnp.float32)
        up_hidden = jnp.dot(expert_rows, up_matrix, preferred_element_type=jnp.float32)
        hidden = (jax.nn.silu(gate_hidden) * up_hidden).astype(jnp.bfloat16)
        return jnp.dot(hidden, down_matrix, preferred_element_type=jnp.float32).astype(jnp.bfloat16)
    outputs = lax.map(one_expert, (per_expert, expert_gate, expert_up, expert_down))
    returned = outputs.reshape(EXPERTS, N_EP, CAP, D).transpose(1, 0, 2, 3).reshape(N_EP, EXPERTS * CAP, D)
    picked = jax.vmap(lambda returned_block, place_row: returned_block[place_row])(returned, places)
    picked = picked.reshape(N_EP * MOE_TOK, TOP_K, D).astype(jnp.float32)
    shares = route_weight / lax.optimization_barrier(jnp.sum(route_weight, axis=-1, keepdims=True))
    return lax.optimization_barrier(jnp.sum(picked * shares[:, :, None], axis=1)).astype(jnp.bfloat16)

def reference(query_input, key_input, value_input, query_gain, key_gain, mixer_out, moe_input, moe_gain, routes, route_weight, expert_gate, expert_up, expert_down):
    seq_len = query_input.shape[0]
    positions = jnp.arange(seq_len, dtype=jnp.int32)
    cosine, sine_table = rope_tables(positions, HEAD_DIM)
    query_heads = query_input.astype(jnp.float32).reshape(seq_len, HEADS, HEAD_DIM)
    key_heads = key_input.astype(jnp.float32).reshape(seq_len, KV_HEADS, HEAD_DIM)
    query_rot = rotate(head_norm(query_heads, query_gain), cosine, sine_table).astype(jnp.bfloat16)
    key_rot = rotate(head_norm(key_heads, key_gain), cosine, sine_table).astype(jnp.bfloat16)
    attended = attend(query_rot, key_rot, value_input)
    attn_mixed = jnp.dot(attended, mixer_out, preferred_element_type=jnp.float32).astype(jnp.bfloat16)
    moe_out = experts_layer(moe_input, moe_gain, routes, route_weight, expert_gate, expert_up, expert_down)
    return (attn_mixed, moe_out)
```

```python
import functools
import math

import jax
import jax.numpy as jnp
from jax import lax
from jax.experimental import pallas as pl
from jax.experimental.pallas import tpu as pltpu
from jax.sharding import PartitionSpec as P

GRID_W = 64
CORES = 2
ONES = 16

epsilon = 1e-06
base_theta = 10000.0


def rope_tables(first_row, grid_rows, head_width, width):
    quarter = head_width // 4
    lane = jnp.arange(width, dtype=jnp.int32)
    inverse = base_theta ** (-(lane % quarter).astype(jnp.float32) / quarter)
    line = jnp.arange(grid_rows + GRID_W, dtype=jnp.int32)
    place = jnp.where(line < grid_rows, first_row + line, line - grid_rows)
    angles = place.astype(jnp.float32)[:, None] * inverse[None, :]
    first = (lane % head_width) < head_width // 2
    sine = jnp.sin(angles)
    return jnp.cos(angles), jnp.where(first[None, :], -sine, sine)


def norm_rotate(columns, gain, gain_swapped, cosine, sine, head_width):
    width = columns.shape[1]
    a = lax.broadcasted_iota(jnp.int32, (width, width), 0)
    b = lax.broadcasted_iota(jnp.int32, (width, width), 1)
    half = head_width // 2
    same_head = jnp.where(a // head_width == b // head_width, 1.0, 0.0)
    partner = jnp.where(b % head_width < half, b + half, b - half)
    swap = jnp.where(a == partner, 1.0, 0.0).astype(jnp.bfloat16)
    values = columns.astype(jnp.float32)
    mean = (
        jnp.dot(
            values * values,
            same_head,
            precision=lax.Precision.HIGHEST,
            preferred_element_type=jnp.float32,
        )
        / head_width
    )
    scale = lax.rsqrt(mean + epsilon)
    swapped = jnp.dot(columns, swap, preferred_element_type=jnp.float32)
    return (
        values * scale * gain * cosine + swapped * scale * gain_swapped * sine
    ).astype(jnp.bfloat16)


def kernel(
    dims,
    x_hbm,
    q_hbm,
    k_hbm,
    v_hbm,
    gate_hbm,
    up_hbm,
    down_hbm,
    mixer_hbm,
    cos_table,
    sin_table,
    q_gain_ref,
    k_gain_ref,
    moe_gain_ref,
    rows_ref,
    weight_ref,
    attn_ref,
    moe_ref,
    x_in,
    q_in,
    k_in,
    v_in,
    normed,
    disp,
    near,
    pick,
    share_ref,
    cos_ref,
    sin_ref,
    q_all,
    k_all,
    v_all,
    incoming,
    hid,
    eo,
    ret,
    att_all,
    mix_acc,
    gate_w,
    up_w,
    down_w,
    mixer_w,
    m_ref,
    acc_ref,
    w_sem,
    d_send,
    d_recv,
    near_sem,
    kv_up,
    kv_down,
    kv_recv,
    f_send,
    f_recv,
    g_send,
    g_recv,
    h_send,
    h_recv,
    r_send,
    r_recv,
    a_send,
    a_recv,
):
    n, T, head_width = dims
    nz = n // CORES
    e = lax.axis_index("ep")
    t = lax.axis_index("tp")
    z = e // CORES
    c = e % CORES
    sibling = z * CORES + (1 - c)
    kh, group_rows, pw = q_all.shape
    rows = q_in.shape[0]
    group = group_rows // rows
    gw = group * head_width
    kw = k_in.shape[1]
    token_count, model_width = x_in.shape
    top = rows_ref.shape[0]
    capp = disp.shape[1]
    feat = disp.shape[2]
    ffl = gate_w.shape[1]
    cols = down_w.shape[1]
    bf = jnp.bfloat16
    f32 = jnp.float32

    loads = [
        pltpu.make_async_copy(src, dst, w_sem.at[i])
        for i, (src, dst) in enumerate(
            [
                (x_hbm, x_in),
                (k_hbm, k_in),
                (v_hbm, v_in),
                (q_hbm, q_in),
                (gate_hbm, gate_w),
                (up_hbm, up_w),
                (down_hbm, down_w),
                (mixer_hbm, mixer_w),
            ]
        )
    ]
    for load in loads:
        load.start()

    barrier = pltpu.get_barrier_semaphore()

    def greet(j, carry):
        pl.semaphore_signal(
            barrier, inc=1, device_id={"ep": (e + j) % n}, device_id_type=pl.DeviceIdType.MESH
        )
        return carry

    lax.fori_loop(1, n, greet, 0)
    for p in range(1, T):
        pl.semaphore_signal(
            barrier, inc=1, device_id={"tp": (t + p) % T}, device_id_type=pl.DeviceIdType.MESH
        )

    low = jnp.minimum(z, nz - 1 - z)
    left = z * 2 < nz

    inner = low > 0

    def line(k):
        outward = ((k + 1) // 2) * (2 * (k % 2) - 1)
        around = jnp.where(left, z - outward, z + outward)
        return jnp.where(k <= 2 * low, around, jnp.where(left, k, nz - 1 - k))

    def chip(k):
        if nz != 4:
            return line(k)
        near = jnp.where(k == 2, 3, jnp.where(k == 3, 2, k))
        return line(jnp.where(inner, near, jnp.where(k == 0, 0, k % 3 + 1)))

    def rdma(src, dst, ss, rs, axis, index):
        return pltpu.make_async_remote_copy(
            src_ref=src,
            dst_ref=dst,
            send_sem=ss,
            recv_sem=rs,
            device_id={axis: index},
            device_id_type=pl.DeviceIdType.MESH,
        )

    class Swap:
        def __init__(self, view, send, recv, k):
            self.view, self.send, self.recv, self.k = view, send, recv, k

        def copy(self, slot, owner, half, peer):
            block = self.view(owner, half)
            return rdma(
                block, block, self.send.at[slot, self.k], self.recv.at[slot, self.k], "tp", peer
            )

        def plan(self):
            x_next, y_next = t + 1 - 2 * (t % 2), (t + 2) % 4
            return [
                (0, t, None, x_next),
                (1, t, None, y_next),
                (2, x_next, 0, y_next),
                (3, y_next, 1, x_next),
            ]

        def start(self):
            if T == 4:
                for slot, owner, half, peer in self.plan()[:2]:
                    self.copy(slot, owner, half, peer).start()
            else:
                for p in range(1, T):
                    self.copy(p - 1, t, None, (t + p) % T).start()

        def relay(self):
            if T == 4:
                x_next, y_next = t + 1 - 2 * (t % 2), (t + 2) % 4
                for first, owner, plan in (
                    (0, x_next, self.plan()[2]),
                    (1, y_next, self.plan()[3]),
                ):
                    self.copy(first, owner, None, owner).wait_recv()
                    self.copy(*plan).start()

        def finish(self):
            if T == 4:
                for slot in (2, 3):
                    self.copy(slot, 3 - t, slot - 2, 3 - t).wait_recv()
            else:
                for p in range(1, T):
                    owner = (t + T - p) % T
                    self.copy(p - 1, owner, None, owner).wait_recv()

        def drain(self):
            if T == 4:
                for slot, owner, half, peer in self.plan():
                    self.copy(slot, owner, half, peer).wait_send()
            else:
                for p in range(1, T):
                    self.copy(p - 1, t, None, (t + p) % T).wait_send()

    def pair_at(k):
        return pl.ds(chip(k) * CORES, CORES)

    def pair_view(buffer, k):
        def view(owner, half):
            if half is None:
                return buffer.at[owner, pair_at(k)]
            return buffer.at[owner, chip(k) * CORES + half]

        return view

    def g_swap(k):
        return Swap(pair_view(incoming, k), g_send, g_recv, k)

    def h_swap(k):
        return Swap(pair_view(hid, k), h_send, h_recv, k)

    def att_view(owner, half):
        if half is None:
            return att_all.at[owner]
        return att_all.at[owner, pl.ds(half * (rows // 2), rows // 2)]

    a_swap = Swap(att_view, a_send, a_recv, 0)

    def d_copy(dest, origin):
        return rdma(
            disp.at[dest], incoming.at[t, origin], d_send.at[dest], d_recv.at[origin], "ep", dest
        )

    near_copy = rdma(near, incoming.at[:, e], near_sem.at[0], near_sem.at[1], "ep", sibling)
    near_in = rdma(near, incoming.at[:, sibling], near_sem.at[0], near_sem.at[1], "ep", sibling)

    def kv_copies(zk, core, send, recv, dest):
        at = pl.ds(pl.multiple_of(core * rows, rows), rows)
        keys = k_all.at[zk, at]
        values = v_all.at[zk, :, 0:head_width, at]
        return [
            rdma(keys, keys, send.at[0, zk], recv.at[0, zk], "ep", dest),
            rdma(values, values, send.at[1, zk], recv.at[1, zk], "ep", dest),
        ]

    def kv_step(zk, direction):
        send = kv_up if direction > 0 else kv_down
        return kv_copies(zk, c, send, kv_recv, (e + direction * CORES + n) % n)

    def kv_across(zk):
        return kv_copies(zk, c, f_send, f_recv, sibling)

    def kv_pass(zk, act):
        @pl.when((zk <= z) & (z + 1 < nz))
        def _():
            for copy in kv_step(zk, 1):
                act(copy)

        @pl.when((zk >= z) & (z > 0))
        def _():
            for copy in kv_step(zk, -1):
                act(copy)

        for copy in kv_across(zk):
            act(copy)

    def places():
        expert = lax.broadcasted_iota(jnp.int32, (n, token_count), 0)
        named = [expert == rows_ref[k : k + 1, :] for k in range(top)]
        count = sum(jnp.where(x, 1.0, 0.0) for x in named).astype(bf)
        i = lax.broadcasted_iota(jnp.int32, (token_count, token_count), 0)
        j = lax.broadcasted_iota(jnp.int32, (token_count, token_count), 1)
        earlier = jnp.dot(
            count, jnp.where(i < j, 1.0, 0.0).astype(bf), preferred_element_type=f32
        )
        by_row = [
            rows_ref[k : k + 1, :].astype(f32) * capp
            + jnp.sum(jnp.where(named[k], earlier, 0.0), axis=0, keepdims=True)
            for k in range(top)
        ]
        width = 128
        weights = [weight_ref[k : k + 1, :] for k in range(top)]
        total = sum(weights)
        lines = by_row + [x / total for x in weights]
        lines.append(jnp.zeros((width - len(lines), token_count), f32))
        by_col = jnp.concatenate(lines, axis=0).T
        return by_row, by_col

    table_width = cos_table.shape[1]
    grid_rows = rows // GRID_W
    lane = lax.broadcasted_iota(jnp.int32, (GRID_W, table_width), 1)
    by_grid_row = (lane // (head_width // 4)) % 2 == 0
    for table, out in ((cos_table, cos_ref), (sin_table, sin_ref)):
        for r in range(grid_rows):
            out[r * GRID_W : (r + 1) * GRID_W] = jnp.where(
                by_grid_row, table[r : r + 1], table[grid_rows:]
            )

    def gain_rows(ref, width):
        gain = ref[...]
        flipped = [gain[:, head_width // 2 :], gain[:, : head_width // 2]]
        times = width // head_width
        return (
            jnp.concatenate([gain] * times, axis=1) if times > 1 else gain,
            jnp.concatenate(flipped * times, axis=1),
        )

    q_gain, q_gain_swapped = gain_rows(q_gain_ref, gw)
    k_gain, k_gain_swapped = gain_rows(k_gain_ref, pw)

    by_row, by_col = places()

    loads[0].wait()
    strip = math.gcd(token_count, 64)

    def normalise(i, carry):
        at = pl.ds(pl.multiple_of(i * strip, strip), strip)
        values = x_in[at].astype(f32)
        inv = lax.rsqrt(jnp.mean(values * values, axis=1, keepdims=True) + epsilon)
        normed[at] = (values * inv * moe_gain_ref[...]).astype(bf)
        return carry

    lax.fori_loop(0, token_count // strip, normalise, 0)

    def chosen(first, count):
        slot = lax.broadcasted_iota(jnp.int32, (count, token_count), 0).astype(f32)
        slot = slot + (first * capp).astype(f32)
        return sum(jnp.where(slot == place, 1.0, 0.0) for place in by_row).astype(bf)

    pl.semaphore_wait(barrier, n - 1 + T - 1)
    own_features = pl.ds(pl.multiple_of(t * feat, feat), feat)

    def make_disp(k, carry):
        part = jnp.dot(
            chosen(chip(k) * CORES, CORES * capp),
            normed[:, own_features],
            preferred_element_type=f32,
        ).astype(bf)
        disp[pair_at(k)] = part.reshape(CORES, capp, feat)
        return carry

    def send_disp(i, carry):
        k = jnp.where(i == 1, 1, nz + 1 - i)
        for cc in range(CORES):
            d_copy(line(k) * CORES + cc, e).start()
        return carry

    lax.fori_loop(1, nz, make_disp, 0)
    lax.fori_loop(1, nz, send_disp, 0)
    loads[1].wait()
    loads[2].wait()
    own_keys = pl.ds(pl.multiple_of(c * rows, rows), rows)
    for p in range(kw // pw):
        lanes = slice(p * pw, (p + 1) * pw)
        k_all[z, own_keys, lanes] = norm_rotate(
            k_in[:, lanes],
            k_gain,
            k_gain_swapped,
            cos_ref[:, :pw],
            sin_ref[:, :pw],
            head_width,
        )
        turned = v_in[:, lanes].astype(f32).T.astype(bf)
        for i in range(pw // head_width):
            v_all[z, p * (pw // head_width) + i, 0:head_width, own_keys] = turned[
                i * head_width : (i + 1) * head_width
            ]

    kv_pass(z, lambda copy: copy.start())

    own_pick = chosen(e, capp)
    sibling_pick = chosen(sibling, capp)
    for s in range(T):
        at = slice(s * feat, (s + 1) * feat)
        near[s] = jnp.dot(sibling_pick, normed[:, at], preferred_element_type=f32).astype(bf)
    near_copy.start()
    for s in range(T):
        at = slice(s * feat, (s + 1) * feat)
        incoming[s, e] = jnp.dot(own_pick, normed[:, at], preferred_element_type=f32).astype(bf)

    def spread(k):
        for cc in range(CORES):
            d_copy(chip(k) * CORES + cc, chip(k) * CORES + cc).wait_recv()
        g_swap(k).start()

    v_all[:, :, head_width:, :] = jnp.ones(
        (nz, kh, v_all.shape[2] - head_width, CORES * rows), bf
    )
    m_ref[...] = jnp.full(m_ref.shape, -jnp.inf, f32)
    acc_ref[...] = jnp.zeros(acc_ref.shape, f32)
    slots = lax.broadcasted_iota(jnp.int32, (token_count, n * capp), 1).astype(f32)
    for k in range(top):
        pick[k] = jnp.where(slots == by_col[:, k : k + 1], 1.0, 0.0).astype(bf)
        share_ref[k] = by_col[:, top + k : top + k + 1]

    loads[3].wait()
    for h in range(kh):
        turned = norm_rotate(
            q_in[:, h * gw : (h + 1) * gw],
            q_gain,
            q_gain_swapped,
            cos_ref[:, :gw],
            sin_ref[:, :gw],
            head_width,
        )
        place = (h * head_width) % pw
        for g in range(group):
            parts = [turned[:, g * head_width : (g + 1) * head_width]]
            if place:
                parts.insert(0, jnp.zeros((rows, place), bf))
            if pw - place - head_width:
                parts.append(jnp.zeros((rows, pw - place - head_width), bf))
            q_all[h, g * rows : (g + 1) * rows] = (
                jnp.concatenate(parts, axis=1) if len(parts) > 1 else parts[0]
            )

    factor = math.log2(math.e) * head_width ** (-0.5)
    step_rows = math.gcd(group_rows, 512)

    def attend(zk):
        def one_head(h, carry):
            lanes = pl.ds(pl.multiple_of((h * head_width) // pw * pw, pw), pw)
            keys = k_all[zk, :, lanes] if kh > 1 else k_all[zk]
            values = v_all[zk, h]

            def scores_at(r):
                return lax.dot_general(
                    keys,
                    q_all[h, r : r + step_rows],
                    (((1,), (1,)), ((), ())),
                    preferred_element_type=f32,
                )

            later = scores_at(0)
            for r in range(0, group_rows, step_rows):
                scores = later
                if r + step_rows < group_rows:
                    later = scores_at(r + step_rows)
                at = slice(r, r + step_rows)
                old = m_ref[h, :, at]
                new = jnp.maximum(old, jnp.max(scores, axis=0, keepdims=True))
                weights = jnp.exp2(scores * factor - new * factor).astype(bf)
                m_ref[h, :, at] = new
                acc_ref[h, :, at] = acc_ref[h, :, at] * jnp.exp2((old - new) * factor) + jnp.dot(
                    values, weights, preferred_element_type=f32
                )
            return carry

        lax.fori_loop(0, kh, one_head, 0)

    def kv_arrive(k):
        zk = line(k)

        @pl.when(zk != z)
        def _():
            for copy in kv_step(zk, 1):
                copy.wait_recv()
            kv_pass(zk, lambda copy: copy.start())

    def kv_join(k):
        for copy in kv_copies(line(k), 1 - c, f_send, f_recv, sibling):
            copy.wait_recv()

    def first_half(k):
        @pl.when(k == 0)
        def _():
            near_in.wait_recv()

        @pl.when(k > 0)
        def _():
            g_swap(k).finish()

        gate = jnp.zeros((CORES * capp, ffl), f32)
        up = jnp.zeros((CORES * capp, ffl), f32)
        for s in range(T):
            piece = incoming[s, pair_at(k)].reshape(CORES * capp, feat)
            at = slice(s * feat, (s + 1) * feat)
            gate = gate + jnp.dot(piece, gate_w[at], preferred_element_type=f32)
            up = up + jnp.dot(piece, up_w[at], preferred_element_type=f32)
        hidden = (gate / (1.0 + jnp.exp(-gate)) * up).astype(bf)
        hid[t, pair_at(k)] = hidden.reshape(CORES, capp, ffl)
        h_swap(k).start()

    def r_copy(dest, origin):
        return rdma(eo.at[dest], ret.at[origin], r_send.at[dest], r_recv.at[origin], "ep", dest)

    def second_half(k):
        h_swap(k).finish()
        total = jnp.zeros((CORES * capp, cols), f32)
        for s in range(T):
            piece = hid[s, pair_at(k)].reshape(CORES * capp, ffl)
            total = total + jnp.dot(
                piece, down_w[s * ffl : (s + 1) * ffl], preferred_element_type=f32
            )
        eo[pair_at(k)] = total.astype(bf).reshape(CORES, capp, cols)

    def send_back(k):
        for cc in range(CORES):
            origin = chip(k) * CORES + cc

            @pl.when(origin != e)
            def _():
                r_copy(origin, e).start()

            @pl.when(origin == e)
            def _():
                ret[origin] = eo[origin]

    def tuned():
        outer = jnp.logical_not(inner)
        spread(1)
        kv_join(0)
        attend(z)
        for load in loads[4:7]:
            load.wait()
        first_half(0)
        g_swap(1).relay()
        spread(2)
        h_swap(0).relay()
        first_half(1)
        spread(3)
        g_swap(2).relay()
        second_half(0)
        send_back(0)
        h_swap(1).relay()
        kv_arrive(1)
        g_swap(3).relay()

        @pl.when(inner)
        def _():
            kv_arrive(2)

        first_half(2)
        second_half(1)
        kv_join(1)
        attend(line(1))

        @pl.when(inner)
        def _():
            kv_arrive(3)

        h_swap(2).relay()
        first_half(3)
        second_half(2)

        @pl.when(inner)
        def _():
            send_back(1)

        @pl.when(outer)
        def _():
            kv_arrive(2)

        h_swap(3).relay()
        second_half(3)
        send_back(3)
        kv_join(2)
        attend(line(2))
        send_back(2)

        @pl.when(outer)
        def _():
            send_back(1)
            kv_arrive(3)

        kv_join(3)
        attend(line(3))

    def general():
        kv_join(0)
        attend(z)
        for load in loads[4:7]:
            load.wait()
        if nz > 1:
            spread(1)

        def step(j, carry):
            @pl.when(j < nz)
            def _():
                first_half(j)

            @pl.when(j + 1 < nz)
            def _():
                g_swap(j + 1).relay()

            @pl.when(j + 2 < nz)
            def _():
                spread(j + 2)

            @pl.when((j >= 1) & (j < nz))
            def _():
                kv_arrive(j)

            @pl.when(j >= 1)
            def _():
                h_swap(j - 1).relay()

            @pl.when(j >= 2)
            def _():
                kv_join(j - 1)
                attend(line(j - 1))

            @pl.when(j >= 1)
            def _():
                second_half(j - 1)
                send_back(j - 1)

            return carry

        lax.fori_loop(0, nz + 1, step, 0)

    if nz == 4:
        tuned()
    else:
        general()

    for h in range(kh):
        done = acc_ref[h, 0:head_width] / acc_ref[h, head_width : head_width + 1]
        done = jnp.concatenate([done[:, g * rows : (g + 1) * rows] for g in range(group)], axis=0)
        att_all[t, :, h * gw : (h + 1) * gw] = done.T.astype(bf)
    a_swap.start()

    loads[7].wait()
    aw = att_all.shape[2]
    out_cols = attn_ref.shape[1]
    half = math.gcd(out_cols, 256)

    def mix(owners, opening, closing):
        def strip_of(i, carry):
            at = pl.ds(pl.multiple_of(i * half, half), half)
            total = jnp.zeros((rows, half), f32) if opening else mix_acc[:, at]
            for s in owners:
                total = total + jnp.dot(
                    att_all[s],
                    mixer_w[pl.ds(pl.multiple_of(s * aw, aw), aw), at],
                    preferred_element_type=f32,
                )
            if closing:
                attn_ref[:, at] = total.astype(bf)
            else:
                mix_acc[:, at] = total
            return carry

        lax.fori_loop(0, out_cols // half, strip_of, 0)

    def gather_experts():
        def wait_ret(j, carry):
            origin = (e + j) % n
            r_copy(origin, origin).wait_recv()
            return carry

        lax.fori_loop(1, n, wait_ret, 0)
        returned = ret[...].reshape(n * capp, cols)
        combined = jnp.zeros(moe_ref.shape, f32)
        for k in range(top):
            combined = combined + share_ref[k] * jnp.dot(
                pick[k], returned, preferred_element_type=f32
            )
        moe_ref[...] = combined.astype(bf)

    mix([t], True, False)
    a_swap.relay()
    if T == 4:
        mix([t + 1 - 2 * (t % 2), (t + 2) % 4], False, False)
    gather_experts()
    a_swap.finish()
    if T == 4:
        mix([3 - t], False, True)
    else:
        mix([(t + p) % T for p in range(1, T)], False, True)

    near_copy.wait_send()

    def drain_ep(j, carry):
        r_copy((e + j) % n, e).wait_send()
        return carry

    lax.fori_loop(1, n, drain_ep, 0)

    def drain(k, carry):
        kv_pass(k, lambda copy: copy.wait_send())
        h_swap(k).drain()

        @pl.when(k > 0)
        def _():
            g_swap(k).drain()
            for cc in range(CORES):
                d_copy(chip(k) * CORES + cc, e).wait_send()

        return carry

    lax.fori_loop(0, nz, drain, 0)
    a_swap.drain()


def on_device(
    n,
    T,
    query_input,
    key_input,
    value_input,
    query_gain,
    key_gain,
    mixer_out,
    moe_input,
    moe_gain,
    routes,
    route_weight,
    expert_gate,
    expert_up,
    expert_down,
):
    rows = query_input.shape[0]
    head_width = query_gain.shape[0]
    heads_here = query_input.shape[1] // head_width
    kw = key_input.shape[1]
    kh = kw // head_width
    group = heads_here // kh
    pw = min(128, kw)
    gw = group * head_width
    width = max(gw, pw)
    assert rows % GRID_W == 0
    grid_rows = rows // GRID_W
    cosine, sine = rope_tables(lax.axis_index("ep") * grid_rows, grid_rows, head_width, width)

    token_count, model_width = moe_input.shape
    top = routes.shape[1]
    local_experts = expert_gate.shape[0]
    assert local_experts == 1
    expert_count = local_experts * n
    capacity = 3 * token_count * top // (2 * expert_count)
    capp = -(-capacity // 16) * 16
    feat = model_width // T
    gate = expert_gate[0]
    up = expert_up[0]
    down = expert_down[0]
    ffl = gate.shape[1]
    cols = down.shape[1]
    nz = n // CORES
    aw = heads_here * head_width
    out_cols = mixer_out.shape[1]
    slots = 4 if T == 4 else T - 1
    bf = jnp.bfloat16
    dma = pltpu.SemaphoreType.DMA
    vmem = pl.BlockSpec(memory_space=pltpu.VMEM)
    hbm = pl.BlockSpec(memory_space=pl.ANY)
    return pl.pallas_call(
        functools.partial(kernel, (n, T, head_width)),
        out_shape=(
            jax.ShapeDtypeStruct((rows, out_cols), bf),
            jax.ShapeDtypeStruct((token_count, cols), bf),
        ),
        in_specs=[hbm] * 8 + [vmem] * 7,
        out_specs=(vmem, vmem),
        scratch_shapes=[
            pltpu.VMEM(moe_input.shape, bf),
            pltpu.VMEM(query_input.shape, bf),
            pltpu.VMEM(key_input.shape, bf),
            pltpu.VMEM(value_input.shape, bf),
            pltpu.VMEM(moe_input.shape, bf),
            pltpu.VMEM((n, capp, feat), bf),
            pltpu.VMEM((T, capp, feat), bf),
            pltpu.VMEM((top, token_count, n * capp), bf),
            pltpu.VMEM((top, token_count, 1), jnp.float32),
            pltpu.VMEM((rows, width), jnp.float32),
            pltpu.VMEM((rows, width), jnp.float32),
            pltpu.VMEM((kh, group * rows, pw), bf),
            pltpu.VMEM((nz, CORES * rows, kw), bf),
            pltpu.VMEM((nz, kh, head_width + ONES, CORES * rows), bf),
            pltpu.VMEM((T, n, capp, feat), bf),
            pltpu.VMEM((T, n, capp, ffl), bf),
            pltpu.VMEM((n, capp, cols), bf),
            pltpu.VMEM((n, capp, cols), bf),
            pltpu.VMEM((T, rows, aw), bf),
            pltpu.VMEM((rows, out_cols), jnp.float32),
            pltpu.VMEM(gate.shape, bf),
            pltpu.VMEM(up.shape, bf),
            pltpu.VMEM(down.shape, bf),
            pltpu.VMEM(mixer_out.shape, bf),
            pltpu.VMEM((kh, 1, group * rows), jnp.float32),
            pltpu.VMEM((kh, head_width + ONES, group * rows), jnp.float32),
            dma((8,)),
            dma((n,)),
            dma((n,)),
            dma((2,)),
            dma((2, nz)),
            dma((2, nz)),
            dma((2, nz)),
            dma((2, nz)),
            dma((2, nz)),
            dma((slots, nz)),
            dma((slots, nz)),
            dma((slots, nz)),
            dma((slots, nz)),
            dma((n,)),
            dma((n,)),
            dma((slots, 1)),
            dma((slots, 1)),
        ],
        compiler_params=pltpu.CompilerParams(
            collective_id=0, has_side_effects=True, vmem_limit_bytes=63 * 1024 * 1024
        ),
    )(
        moe_input,
        query_input,
        key_input,
        value_input,
        gate,
        up,
        down,
        mixer_out,
        cosine,
        sine,
        query_gain[None, :],
        key_gain[None, :],
        moe_gain[None, :],
        routes.T,
        route_weight.T,
    )


def solution(mesh):
    placed = (
        P("ep", "tp"),
        P("ep", "tp"),
        P("ep", "tp"),
        P(),
        P(),
        P(None, "tp"),
        P("ep", None),
        P(),
        P("ep", None),
        P("ep", None),
        P("ep", None, "tp"),
        P("ep", None, "tp"),
        P("ep", None, "tp"),
    )
    return jax.shard_map(
        functools.partial(on_device, mesh.shape["ep"], mesh.shape["tp"]),
        mesh=mesh,
        in_specs=placed,
        out_specs=(P("ep", "tp"), P("ep", "tp")),
        check_vma=False,
    )
```

```python
import functools
import math

import jax
import jax.numpy as jnp
from jax import lax
from jax.experimental import pallas as pl
from jax.experimental.pallas import tpu as pltpu
from jax.sharding import PartitionSpec as P

GRID_W = 64
CORES = 2
ONES = 16

epsilon = 1e-06
base_theta = 10000.0


def rope_tables(first_row, grid_rows, head_width, width):
    quarter = head_width // 4
    lane = jnp.arange(width, dtype=jnp.int32)
    inverse = base_theta ** (-(lane % quarter).astype(jnp.float32) / quarter)
    line = jnp.arange(grid_rows + GRID_W, dtype=jnp.int32)
    place = jnp.where(line < grid_rows, first_row + line, line - grid_rows)
    angles = place.astype(jnp.float32)[:, None] * inverse[None, :]
    first = (lane % head_width) < head_width // 2
    sine = jnp.sin(angles)
    return jnp.cos(angles), jnp.where(first[None, :], -sine, sine)


def norm_rotate(columns, gain, gain_swapped, cosine, sine, head_width):
    width = columns.shape[1]
    a = lax.broadcasted_iota(jnp.int32, (width, width), 0)
    b = lax.broadcasted_iota(jnp.int32, (width, width), 1)
    half = head_width // 2
    same_head = jnp.where(a // head_width == b // head_width, 1.0, 0.0)
    partner = jnp.where(b % head_width < half, b + half, b - half)
    swap = jnp.where(a == partner, 1.0, 0.0).astype(jnp.bfloat16)
    values = columns.astype(jnp.float32)
    mean = (
        jnp.dot(
            values * values,
            same_head,
            precision=lax.Precision.HIGHEST,
            preferred_element_type=jnp.float32,
        )
        / head_width
    )
    scale = lax.rsqrt(mean + epsilon)
    swapped = jnp.dot(columns, swap, preferred_element_type=jnp.float32)
    return (
        values * scale * gain * cosine + swapped * scale * gain_swapped * sine
    ).astype(jnp.bfloat16)


def kernel(
    dims,
    x_hbm,
    q_hbm,
    k_hbm,
    v_hbm,
    gate_hbm,
    up_hbm,
    down_hbm,
    mixer_hbm,
    cos_table,
    sin_table,
    q_gain_ref,
    k_gain_ref,
    moe_gain_ref,
    rows_ref,
    weight_ref,
    attn_hbm,
    moe_hbm,
    attn_ref,
    moe_ref,
    o_sem,
    x_in,
    q_in,
    k_in,
    v_in,
    normed,
    disp,
    near,
    pick,
    share_ref,
    cos_ref,
    sin_ref,
    q_all,
    k_all,
    v_all,
    incoming,
    hid,
    eo,
    ret,
    att_all,
    mix_acc,
    gate_w,
    up_w,
    down_w,
    mixer_w,
    m_ref,
    acc_ref,
    w_sem,
    d_send,
    d_recv,
    near_sem,
    kv_up,
    kv_down,
    kv_recv,
    f_send,
    f_recv,
    g_send,
    g_recv,
    h_send,
    h_recv,
    r_send,
    r_recv,
    a_send,
    a_recv,
):
    n, T, head_width = dims
    nz = n // CORES
    e = lax.axis_index("ep")
    t = lax.axis_index("tp")
    z = e // CORES
    c = e % CORES
    sibling = z * CORES + (1 - c)
    kh, group_rows, pw = q_all.shape
    rows = q_in.shape[0]
    group = group_rows // rows
    gw = group * head_width
    kw = k_in.shape[1]
    token_count, model_width = x_in.shape
    top = rows_ref.shape[0]
    capp = disp.shape[1]
    feat = disp.shape[2]
    ffl = gate_w.shape[1]
    cols = down_w.shape[1]
    bf = jnp.bfloat16
    f32 = jnp.float32

    loads = [
        pltpu.make_async_copy(src, dst, w_sem.at[i])
        for i, (src, dst) in enumerate(
            [
                (x_hbm, x_in),
                (k_hbm, k_in),
                (v_hbm, v_in),
                (q_hbm, q_in),
                (gate_hbm, gate_w),
                (up_hbm, up_w),
                (down_hbm, down_w),
                (mixer_hbm, mixer_w),
            ]
        )
    ]
    for load in loads:
        load.start()

    barrier = pltpu.get_barrier_semaphore()

    def greet(j, carry):
        pl.semaphore_signal(
            barrier, inc=1, device_id={"ep": (e + j) % n}, device_id_type=pl.DeviceIdType.MESH
        )
        return carry

    lax.fori_loop(1, n, greet, 0)
    for p in range(1, T):
        pl.semaphore_signal(
            barrier, inc=1, device_id={"tp": (t + p) % T}, device_id_type=pl.DeviceIdType.MESH
        )

    low = jnp.minimum(z, nz - 1 - z)
    left = z * 2 < nz

    inner = low > 0

    def line(k):
        outward = ((k + 1) // 2) * (2 * (k % 2) - 1)
        around = jnp.where(left, z - outward, z + outward)
        return jnp.where(k <= 2 * low, around, jnp.where(left, k, nz - 1 - k))

    def chip(k):
        if nz != 4:
            return line(k)
        near = jnp.where(k == 2, 3, jnp.where(k == 3, 2, k))
        return line(jnp.where(inner, near, jnp.where(k == 0, 0, k % 3 + 1)))

    def rdma(src, dst, ss, rs, axis, index):
        return pltpu.make_async_remote_copy(
            src_ref=src,
            dst_ref=dst,
            send_sem=ss,
            recv_sem=rs,
            device_id={axis: index},
            device_id_type=pl.DeviceIdType.MESH,
        )

    class Swap:
        def __init__(self, view, send, recv, k):
            self.view, self.send, self.recv, self.k = view, send, recv, k

        def copy(self, slot, owner, half, peer):
            block = self.view(owner, half)
            return rdma(
                block, block, self.send.at[slot, self.k], self.recv.at[slot, self.k], "tp", peer
            )

        def plan(self):
            x_next, y_next = t + 1 - 2 * (t % 2), (t + 2) % 4
            return [
                (0, t, None, x_next),
                (1, t, None, y_next),
                (2, x_next, 0, y_next),
                (3, y_next, 1, x_next),
            ]

        def start(self):
            if T == 4:
                for slot, owner, half, peer in self.plan()[:2]:
                    self.copy(slot, owner, half, peer).start()
            else:
                for p in range(1, T):
                    self.copy(p - 1, t, None, (t + p) % T).start()

        def relay(self):
            if T == 4:
                x_next, y_next = t + 1 - 2 * (t % 2), (t + 2) % 4
                for first, owner, plan in (
                    (0, x_next, self.plan()[2]),
                    (1, y_next, self.plan()[3]),
                ):
                    self.copy(first, owner, None, owner).wait_recv()
                    self.copy(*plan).start()

        def finish(self):
            if T == 4:
                for slot in (2, 3):
                    self.copy(slot, 3 - t, slot - 2, 3 - t).wait_recv()
            else:
                for p in range(1, T):
                    owner = (t + T - p) % T
                    self.copy(p - 1, owner, None, owner).wait_recv()

        def drain(self):
            if T == 4:
                for slot, owner, half, peer in self.plan():
                    self.copy(slot, owner, half, peer).wait_send()
            else:
                for p in range(1, T):
                    self.copy(p - 1, t, None, (t + p) % T).wait_send()

    def pair_at(k):
        return pl.ds(chip(k) * CORES, CORES)

    def pair_view(buffer, k):
        def view(owner, half):
            if half is None:
                return buffer.at[owner, pair_at(k)]
            return buffer.at[owner, chip(k) * CORES + half]

        return view

    def g_swap(k):
        return Swap(pair_view(incoming, k), g_send, g_recv, k)

    def h_swap(k):
        return Swap(pair_view(hid, k), h_send, h_recv, k)

    def a_swap(part):
        def view(owner, half):
            if half is None:
                return att_all.at[owner, part]
            return att_all.at[owner, part, pl.ds(half * (rows // 2), rows // 2)]

        return Swap(view, a_send, a_recv, part)

    def d_copy(dest, origin):
        return rdma(
            disp.at[dest], incoming.at[t, origin], d_send.at[dest], d_recv.at[origin], "ep", dest
        )

    near_copy = rdma(near, incoming.at[:, e], near_sem.at[0], near_sem.at[1], "ep", sibling)
    near_in = rdma(near, incoming.at[:, sibling], near_sem.at[0], near_sem.at[1], "ep", sibling)

    def kv_copies(zk, core, send, recv, dest):
        at = pl.ds(pl.multiple_of(core * rows, rows), rows)
        keys = k_all.at[zk, at]
        values = v_all.at[zk, :, 0:head_width, at]
        return [
            rdma(keys, keys, send.at[0, zk], recv.at[0, zk], "ep", dest),
            rdma(values, values, send.at[1, zk], recv.at[1, zk], "ep", dest),
        ]

    def kv_step(zk, direction):
        send = kv_up if direction > 0 else kv_down
        return kv_copies(zk, c, send, kv_recv, (e + direction * CORES + n) % n)

    def kv_across(zk):
        return kv_copies(zk, c, f_send, f_recv, sibling)

    def kv_pass(zk, act):
        @pl.when((zk <= z) & (z + 1 < nz))
        def _():
            for copy in kv_step(zk, 1):
                act(copy)

        @pl.when((zk >= z) & (z > 0))
        def _():
            for copy in kv_step(zk, -1):
                act(copy)

        for copy in kv_across(zk):
            act(copy)

    def places():
        expert = lax.broadcasted_iota(jnp.int32, (n, token_count), 0)
        named = [expert == rows_ref[k : k + 1, :] for k in range(top)]
        count = sum(jnp.where(x, 1.0, 0.0) for x in named).astype(bf)
        i = lax.broadcasted_iota(jnp.int32, (token_count, token_count), 0)
        j = lax.broadcasted_iota(jnp.int32, (token_count, token_count), 1)
        earlier = jnp.dot(
            count, jnp.where(i < j, 1.0, 0.0).astype(bf), preferred_element_type=f32
        )
        by_row = [
            rows_ref[k : k + 1, :].astype(f32) * capp
            + jnp.sum(jnp.where(named[k], earlier, 0.0), axis=0, keepdims=True)
            for k in range(top)
        ]
        width = 128
        weights = [weight_ref[k : k + 1, :] for k in range(top)]
        total = sum(weights)
        lines = by_row + [x / total for x in weights]
        lines.append(jnp.zeros((width - len(lines), token_count), f32))
        by_col = jnp.concatenate(lines, axis=0).T
        return by_row, by_col

    table_width = cos_table.shape[1]
    grid_rows = rows // GRID_W
    lane = lax.broadcasted_iota(jnp.int32, (GRID_W, table_width), 1)
    by_grid_row = (lane // (head_width // 4)) % 2 == 0
    for table, out in ((cos_table, cos_ref), (sin_table, sin_ref)):
        for r in range(grid_rows):
            out[r * GRID_W : (r + 1) * GRID_W] = jnp.where(
                by_grid_row, table[r : r + 1], table[grid_rows:]
            )

    def gain_rows(ref, width):
        gain = ref[...]
        flipped = [gain[:, head_width // 2 :], gain[:, : head_width // 2]]
        times = width // head_width
        return (
            jnp.concatenate([gain] * times, axis=1) if times > 1 else gain,
            jnp.concatenate(flipped * times, axis=1),
        )

    q_gain, q_gain_swapped = gain_rows(q_gain_ref, gw)
    k_gain, k_gain_swapped = gain_rows(k_gain_ref, pw)

    by_row, by_col = places()

    loads[0].wait()
    strip = math.gcd(token_count, 64)

    def normalise(i, carry):
        at = pl.ds(pl.multiple_of(i * strip, strip), strip)
        values = x_in[at].astype(f32)
        inv = lax.rsqrt(jnp.mean(values * values, axis=1, keepdims=True) + epsilon)
        normed[at] = (values * inv * moe_gain_ref[...]).astype(bf)
        return carry

    lax.fori_loop(0, token_count // strip, normalise, 0)

    def chosen(first, count):
        slot = lax.broadcasted_iota(jnp.int32, (count, token_count), 0).astype(f32)
        slot = slot + (first * capp).astype(f32)
        return sum(jnp.where(slot == place, 1.0, 0.0) for place in by_row).astype(bf)

    pl.semaphore_wait(barrier, n - 1 + T - 1)
    own_features = pl.ds(pl.multiple_of(t * feat, feat), feat)

    def make_disp(k, carry):
        part = jnp.dot(
            chosen(chip(k) * CORES, CORES * capp),
            normed[:, own_features],
            preferred_element_type=f32,
        ).astype(bf)
        disp[pair_at(k)] = part.reshape(CORES, capp, feat)
        return carry

    def send_disp(i, carry):
        k = jnp.where(i == 1, 1, nz + 1 - i)
        for cc in range(CORES):
            d_copy(line(k) * CORES + cc, e).start()
        return carry

    lax.fori_loop(1, nz, make_disp, 0)
    lax.fori_loop(1, nz, send_disp, 0)
    loads[1].wait()
    loads[2].wait()
    own_keys = pl.ds(pl.multiple_of(c * rows, rows), rows)
    for p in range(kw // pw):
        lanes = slice(p * pw, (p + 1) * pw)
        k_all[z, own_keys, lanes] = norm_rotate(
            k_in[:, lanes],
            k_gain,
            k_gain_swapped,
            cos_ref[:, :pw],
            sin_ref[:, :pw],
            head_width,
        )
        turned = v_in[:, lanes].astype(f32).T.astype(bf)
        for i in range(pw // head_width):
            v_all[z, p * (pw // head_width) + i, 0:head_width, own_keys] = turned[
                i * head_width : (i + 1) * head_width
            ]

    kv_pass(z, lambda copy: copy.start())

    own_pick = chosen(e, capp)
    sibling_pick = chosen(sibling, capp)
    for s in range(T):
        at = slice(s * feat, (s + 1) * feat)
        near[s] = jnp.dot(sibling_pick, normed[:, at], preferred_element_type=f32).astype(bf)
    near_copy.start()
    for s in range(T):
        at = slice(s * feat, (s + 1) * feat)
        incoming[s, e] = jnp.dot(own_pick, normed[:, at], preferred_element_type=f32).astype(bf)

    def spread(k):
        for cc in range(CORES):
            d_copy(chip(k) * CORES + cc, chip(k) * CORES + cc).wait_recv()
        g_swap(k).start()

    v_all[:, :, head_width:, :] = jnp.ones(
        (nz, kh, v_all.shape[2] - head_width, CORES * rows), bf
    )
    m_ref[...] = jnp.full(m_ref.shape, -jnp.inf, f32)
    acc_ref[...] = jnp.zeros(acc_ref.shape, f32)
    slots = lax.broadcasted_iota(jnp.int32, (token_count, n * capp), 1).astype(f32)
    for k in range(top):
        pick[k] = jnp.where(slots == by_col[:, k : k + 1], 1.0, 0.0).astype(bf)
        share_ref[k] = by_col[:, top + k : top + k + 1]

    loads[3].wait()
    for h in range(kh):
        turned = norm_rotate(
            q_in[:, h * gw : (h + 1) * gw],
            q_gain,
            q_gain_swapped,
            cos_ref[:, :gw],
            sin_ref[:, :gw],
            head_width,
        )
        place = (h * head_width) % pw
        for g in range(group):
            parts = [turned[:, g * head_width : (g + 1) * head_width]]
            if place:
                parts.insert(0, jnp.zeros((rows, place), bf))
            if pw - place - head_width:
                parts.append(jnp.zeros((rows, pw - place - head_width), bf))
            q_all[h, g * rows : (g + 1) * rows] = (
                jnp.concatenate(parts, axis=1) if len(parts) > 1 else parts[0]
            )

    factor = math.log2(math.e) * head_width ** (-0.5)
    step_rows = math.gcd(group_rows, 512)

    parts = att_all.shape[1]
    heads_part = kh // parts

    def attend(zk, first=0, last=kh):
        def one_head(h, carry):
            lanes = pl.ds(pl.multiple_of((h * head_width) // pw * pw, pw), pw)
            keys = k_all[zk, :, lanes] if kh > 1 else k_all[zk]
            values = v_all[zk, h]

            def scores_at(r):
                return lax.dot_general(
                    keys,
                    q_all[h, r : r + step_rows],
                    (((1,), (1,)), ((), ())),
                    preferred_element_type=f32,
                )

            later = scores_at(0)
            for r in range(0, group_rows, step_rows):
                scores = later
                if r + step_rows < group_rows:
                    later = scores_at(r + step_rows)
                at = slice(r, r + step_rows)
                old = m_ref[h, :, at]
                new = jnp.maximum(old, jnp.max(scores, axis=0, keepdims=True))
                weights = jnp.exp2(scores * factor - new * factor).astype(bf)
                m_ref[h, :, at] = new
                acc_ref[h, :, at] = acc_ref[h, :, at] * jnp.exp2((old - new) * factor) + jnp.dot(
                    values, weights, preferred_element_type=f32
                )
            return carry

        lax.fori_loop(first, last, one_head, 0)

    def kv_arrive(k):
        zk = line(k)

        @pl.when(zk != z)
        def _():
            for copy in kv_step(zk, 1):
                copy.wait_recv()
            kv_pass(zk, lambda copy: copy.start())

    def kv_join(k):
        for copy in kv_copies(line(k), 1 - c, f_send, f_recv, sibling):
            copy.wait_recv()

    def first_half(k):
        @pl.when(k == 0)
        def _():
            near_in.wait_recv()

        @pl.when(k > 0)
        def _():
            g_swap(k).finish()

        gate = jnp.zeros((CORES * capp, ffl), f32)
        up = jnp.zeros((CORES * capp, ffl), f32)
        for s in range(T):
            piece = incoming[s, pair_at(k)].reshape(CORES * capp, feat)
            at = slice(s * feat, (s + 1) * feat)
            gate = gate + jnp.dot(piece, gate_w[at], preferred_element_type=f32)
            up = up + jnp.dot(piece, up_w[at], preferred_element_type=f32)
        hidden = (gate / (1.0 + jnp.exp(-gate)) * up).astype(bf)
        hid[t, pair_at(k)] = hidden.reshape(CORES, capp, ffl)
        h_swap(k).start()

    def r_copy(dest, origin):
        return rdma(eo.at[dest], ret.at[origin], r_send.at[dest], r_recv.at[origin], "ep", dest)

    def second_half(k):
        h_swap(k).finish()
        total = jnp.zeros((CORES * capp, cols), f32)
        for s in range(T):
            piece = hid[s, pair_at(k)].reshape(CORES * capp, ffl)
            total = total + jnp.dot(
                piece, down_w[s * ffl : (s + 1) * ffl], preferred_element_type=f32
            )
        eo[pair_at(k)] = total.astype(bf).reshape(CORES, capp, cols)

    def send_back(k):
        for cc in range(CORES):
            origin = chip(k) * CORES + cc

            @pl.when(origin != e)
            def _():
                r_copy(origin, e).start()

            @pl.when(origin == e)
            def _():
                ret[origin] = eo[origin]

    def finish_heads(part):
        for i in range(heads_part):
            h = part * heads_part + i
            done = acc_ref[h, 0:head_width] / acc_ref[h, head_width : head_width + 1]
            done = jnp.concatenate(
                [done[:, g * rows : (g + 1) * rows] for g in range(group)], axis=0
            )
            att_all[t, part, :, i * gw : (i + 1) * gw] = done.T.astype(bf)
        a_swap(part).start()

    def tuned():
        outer = jnp.logical_not(inner)
        spread(1)
        kv_join(0)
        attend(z)
        for load in loads[4:7]:
            load.wait()
        first_half(0)
        g_swap(1).relay()
        spread(2)
        h_swap(0).relay()
        first_half(1)
        spread(3)
        g_swap(2).relay()
        second_half(0)
        send_back(0)
        h_swap(1).relay()
        kv_arrive(1)
        kv_join(1)
        attend(line(1), 0, kh // 2)

        @pl.when(inner)
        def _():
            kv_arrive(2)

        @pl.when(outer)
        def _():
            attend(line(1), kh // 2, kh)

        g_swap(3).relay()

        @pl.when(inner)
        def _():
            attend(line(1), kh // 2, kh)

        first_half(2)
        second_half(1)

        @pl.when(inner)
        def _():
            kv_arrive(3)
            send_back(1)

        h_swap(2).relay()
        first_half(3)

        @pl.when(outer)
        def _():
            send_back(1)

        second_half(2)

        @pl.when(outer)
        def _():
            kv_arrive(2)

        h_swap(3).relay()
        kv_join(2)
        attend(line(2), 0, kh // 2)
        second_half(3)
        send_back(3)
        attend(line(2), kh // 2, kh)
        send_back(2)

        @pl.when(outer)
        def _():
            kv_arrive(3)

        kv_join(3)
        for part in range(parts):
            attend(line(3), part * heads_part, (part + 1) * heads_part)
            finish_heads(part)

    def general():
        kv_join(0)
        attend(z)
        for load in loads[4:7]:
            load.wait()
        if nz > 1:
            spread(1)

        def step(j, carry):
            @pl.when(j < nz)
            def _():
                first_half(j)

            @pl.when(j + 1 < nz)
            def _():
                g_swap(j + 1).relay()

            @pl.when(j + 2 < nz)
            def _():
                spread(j + 2)

            @pl.when((j >= 1) & (j < nz))
            def _():
                kv_arrive(j)

            @pl.when(j >= 1)
            def _():
                h_swap(j - 1).relay()

            @pl.when(j >= 2)
            def _():
                kv_join(j - 1)
                attend(line(j - 1))

            @pl.when(j >= 1)
            def _():
                second_half(j - 1)
                send_back(j - 1)

            return carry

        lax.fori_loop(0, nz + 1, step, 0)
        for part in range(parts):
            finish_heads(part)

    if nz == 4:
        tuned()
    else:
        general()

    loads[7].wait()
    aw = parts * att_all.shape[3]
    out_cols = attn_ref.shape[1]
    half = math.gcd(out_cols, 256)

    def strip_out(i):
        at = pl.ds(pl.multiple_of(i * half, half), half)
        return pltpu.make_async_copy(attn_ref.at[:, at], attn_hbm.at[:, at], o_sem.at[i + 1])

    moe_out = pltpu.make_async_copy(moe_ref, moe_hbm, o_sem.at[0])

    def mix(owners, opening, closing):
        def strip_of(i, carry):
            at = pl.ds(pl.multiple_of(i * half, half), half)
            total = jnp.zeros((rows, half), f32) if opening else mix_acc[:, at]
            for s in owners:
                for part in range(parts):
                    width = aw // parts
                    lines = pl.ds(pl.multiple_of(s * aw + part * width, width), width)
                    total = total + jnp.dot(
                        att_all[s, part], mixer_w[lines, at], preferred_element_type=f32
                    )
            if closing:
                attn_ref[:, at] = total.astype(bf)
                strip_out(i).start()
            else:
                mix_acc[:, at] = total
            return carry

        lax.fori_loop(0, out_cols // half, strip_of, 0)

    def gather_experts():
        def wait_ret(j, carry):
            origin = (e + j) % n
            r_copy(origin, origin).wait_recv()
            return carry

        lax.fori_loop(1, n, wait_ret, 0)
        returned = ret[...].reshape(n * capp, cols)
        combined = jnp.zeros(moe_ref.shape, f32)
        for k in range(top):
            combined = combined + share_ref[k] * jnp.dot(
                pick[k], returned, preferred_element_type=f32
            )
        moe_ref[...] = combined.astype(bf)
        moe_out.start()

    mix([t], True, False)
    for part in range(parts):
        a_swap(part).relay()
    if T == 4:
        mix([t + 1 - 2 * (t % 2), (t + 2) % 4], False, False)
    gather_experts()
    for part in range(parts):
        a_swap(part).finish()
    if T == 4:
        mix([3 - t], False, True)
    else:
        mix([(t + p) % T for p in range(1, T)], False, True)

    near_copy.wait_send()

    def drain_ep(j, carry):
        r_copy((e + j) % n, e).wait_send()
        return carry

    lax.fori_loop(1, n, drain_ep, 0)

    def drain(k, carry):
        kv_pass(k, lambda copy: copy.wait_send())
        h_swap(k).drain()

        @pl.when(k > 0)
        def _():
            g_swap(k).drain()
            for cc in range(CORES):
                d_copy(chip(k) * CORES + cc, e).wait_send()

        return carry

    lax.fori_loop(0, nz, drain, 0)
    for part in range(parts):
        a_swap(part).drain()
    moe_out.wait()

    def drain_out(i, carry):
        strip_out(i).wait()
        return carry

    lax.fori_loop(0, out_cols // half, drain_out, 0)


def on_device(
    n,
    T,
    query_input,
    key_input,
    value_input,
    query_gain,
    key_gain,
    mixer_out,
    moe_input,
    moe_gain,
    routes,
    route_weight,
    expert_gate,
    expert_up,
    expert_down,
):
    rows = query_input.shape[0]
    head_width = query_gain.shape[0]
    heads_here = query_input.shape[1] // head_width
    kw = key_input.shape[1]
    kh = kw // head_width
    group = heads_here // kh
    pw = min(128, kw)
    gw = group * head_width
    width = max(gw, pw)
    assert rows % GRID_W == 0
    grid_rows = rows // GRID_W
    cosine, sine = rope_tables(lax.axis_index("ep") * grid_rows, grid_rows, head_width, width)

    token_count, model_width = moe_input.shape
    top = routes.shape[1]
    local_experts = expert_gate.shape[0]
    assert local_experts == 1
    expert_count = local_experts * n
    capacity = 3 * token_count * top // (2 * expert_count)
    capp = -(-capacity // 16) * 16
    feat = model_width // T
    gate = expert_gate[0]
    up = expert_up[0]
    down = expert_down[0]
    ffl = gate.shape[1]
    cols = down.shape[1]
    nz = n // CORES
    aw = heads_here * head_width
    out_cols = mixer_out.shape[1]
    slots = 4 if T == 4 else T - 1
    parts = kh
    bf = jnp.bfloat16
    dma = pltpu.SemaphoreType.DMA
    vmem = pl.BlockSpec(memory_space=pltpu.VMEM)
    hbm = pl.BlockSpec(memory_space=pl.ANY)
    return pl.pallas_call(
        functools.partial(kernel, (n, T, head_width)),
        out_shape=(
            jax.ShapeDtypeStruct((rows, out_cols), bf),
            jax.ShapeDtypeStruct((token_count, cols), bf),
        ),
        in_specs=[hbm] * 8 + [vmem] * 7,
        out_specs=(hbm, hbm),
        scratch_shapes=[
            pltpu.VMEM((rows, out_cols), bf),
            pltpu.VMEM((token_count, cols), bf),
            dma((1 + out_cols // math.gcd(out_cols, 256),)),
            pltpu.VMEM(moe_input.shape, bf),
            pltpu.VMEM(query_input.shape, bf),
            pltpu.VMEM(key_input.shape, bf),
            pltpu.VMEM(value_input.shape, bf),
            pltpu.VMEM(moe_input.shape, bf),
            pltpu.VMEM((n, capp, feat), bf),
            pltpu.VMEM((T, capp, feat), bf),
            pltpu.VMEM((top, token_count, n * capp), bf),
            pltpu.VMEM((top, token_count, 1), jnp.float32),
            pltpu.VMEM((rows, width), jnp.float32),
            pltpu.VMEM((rows, width), jnp.float32),
            pltpu.VMEM((kh, group * rows, pw), bf),
            pltpu.VMEM((nz, CORES * rows, kw), bf),
            pltpu.VMEM((nz, kh, head_width + ONES, CORES * rows), bf),
            pltpu.VMEM((T, n, capp, feat), bf),
            pltpu.VMEM((T, n, capp, ffl), bf),
            pltpu.VMEM((n, capp, cols), bf),
            pltpu.VMEM((n, capp, cols), bf),
            pltpu.VMEM((T, parts, rows, aw // parts), bf),
            pltpu.VMEM((rows, out_cols), jnp.float32),
            pltpu.VMEM(gate.shape, bf),
            pltpu.VMEM(up.shape, bf),
            pltpu.VMEM(down.shape, bf),
            pltpu.VMEM(mixer_out.shape, bf),
            pltpu.VMEM((kh, 1, group * rows), jnp.float32),
            pltpu.VMEM((kh, head_width + ONES, group * rows), jnp.float32),
            dma((8,)),
            dma((n,)),
            dma((n,)),
            dma((2,)),
            dma((2, nz)),
            dma((2, nz)),
            dma((2, nz)),
            dma((2, nz)),
            dma((2, nz)),
            dma((slots, nz)),
            dma((slots, nz)),
            dma((slots, nz)),
            dma((slots, nz)),
            dma((n,)),
            dma((n,)),
            dma((slots, parts)),
            dma((slots, parts)),
        ],
        compiler_params=pltpu.CompilerParams(
            collective_id=0, has_side_effects=True, vmem_limit_bytes=63 * 1024 * 1024
        ),
    )(
        moe_input,
        query_input,
        key_input,
        value_input,
        gate,
        up,
        down,
        mixer_out,
        cosine,
        sine,
        query_gain[None, :],
        key_gain[None, :],
        moe_gain[None, :],
        routes.T,
        route_weight.T,
    )


def solution(mesh):
    placed = (
        P("ep", "tp"),
        P("ep", "tp"),
        P("ep", "tp"),
        P(),
        P(),
        P(None, "tp"),
        P("ep", None),
        P(),
        P("ep", None),
        P("ep", None),
        P("ep", None, "tp"),
        P("ep", None, "tp"),
        P("ep", None, "tp"),
    )
    return jax.shard_map(
        functools.partial(on_device, mesh.shape["ep"], mesh.shape["tp"]),
        mesh=mesh,
        in_specs=placed,
        out_specs=(P("ep", "tp"), P("ep", "tp")),
        check_vma=False,
    )
```

```python
import functools
import math

import jax
import jax.numpy as jnp
from jax import lax
from jax.experimental import pallas as pl
from jax.experimental.pallas import tpu as pltpu
from jax.sharding import PartitionSpec as P

GRID_W = 64
CORES = 2
ONES = 16

epsilon = 1e-06
base_theta = 10000.0


def rope_tables(first_row, grid_rows, head_width, width):
    quarter = head_width // 4
    lane = jnp.arange(width, dtype=jnp.int32)
    inverse = base_theta ** (-(lane % quarter).astype(jnp.float32) / quarter)
    line = jnp.arange(grid_rows + GRID_W, dtype=jnp.int32)
    place = jnp.where(line < grid_rows, first_row + line, line - grid_rows)
    angles = place.astype(jnp.float32)[:, None] * inverse[None, :]
    first = (lane % head_width) < head_width // 2
    sine = jnp.sin(angles)
    return jnp.cos(angles), jnp.where(first[None, :], -sine, sine)


def norm_rotate(columns, gain, gain_swapped, cosine, sine, head_width):
    width = columns.shape[1]
    a = lax.broadcasted_iota(jnp.int32, (width, width), 0)
    b = lax.broadcasted_iota(jnp.int32, (width, width), 1)
    half = head_width // 2
    same_head = jnp.where(a // head_width == b // head_width, 1.0, 0.0)
    partner = jnp.where(b % head_width < half, b + half, b - half)
    swap = jnp.where(a == partner, 1.0, 0.0).astype(jnp.bfloat16)
    values = columns.astype(jnp.float32)
    mean = (
        jnp.dot(
            values * values,
            same_head,
            precision=lax.Precision.HIGHEST,
            preferred_element_type=jnp.float32,
        )
        / head_width
    )
    scale = lax.rsqrt(mean + epsilon)
    swapped = jnp.dot(columns, swap, preferred_element_type=jnp.float32)
    return (
        values * scale * gain * cosine + swapped * scale * gain_swapped * sine
    ).astype(jnp.bfloat16)


def kernel(
    dims,
    x_hbm,
    q_hbm,
    k_hbm,
    v_hbm,
    gate_hbm,
    up_hbm,
    down_hbm,
    mixer_hbm,
    cos_table,
    sin_table,
    q_gain_ref,
    k_gain_ref,
    moe_gain_ref,
    rows_ref,
    weight_ref,
    attn_hbm,
    moe_hbm,
    attn_ref,
    moe_ref,
    o_sem,
    x_in,
    q_in,
    k_in,
    v_in,
    normed,
    disp,
    near,
    pick,
    share_ref,
    cos_ref,
    sin_ref,
    q_all,
    k_all,
    v_all,
    incoming,
    hid,
    eo,
    ret,
    att_all,
    mix_acc,
    gate_w,
    up_w,
    down_w,
    mixer_w,
    m_ref,
    acc_ref,
    w_sem,
    d_send,
    d_recv,
    near_sem,
    kv_up,
    kv_down,
    kv_recv,
    f_send,
    f_recv,
    g_send,
    g_recv,
    h_send,
    h_recv,
    r_send,
    r_recv,
    a_send,
    a_recv,
):
    n, T, head_width = dims
    nz = n // CORES
    e = lax.axis_index("ep")
    t = lax.axis_index("tp")
    z = e // CORES
    c = e % CORES
    sibling = z * CORES + (1 - c)
    kh, group_rows, pw = q_all.shape
    rows = q_in.shape[0]
    group = group_rows // rows
    gw = group * head_width
    kw = k_in.shape[1]
    token_count, model_width = x_in.shape
    top = rows_ref.shape[0]
    capp = disp.shape[1]
    feat = disp.shape[2]
    ffl = gate_w.shape[1]
    cols = down_w.shape[1]
    bf = jnp.bfloat16
    f32 = jnp.float32

    loads = [
        pltpu.make_async_copy(src, dst, w_sem.at[i])
        for i, (src, dst) in enumerate(
            [
                (x_hbm, x_in),
                (k_hbm, k_in),
                (v_hbm, v_in),
                (q_hbm, q_in),
                (gate_hbm, gate_w),
                (up_hbm, up_w),
                (down_hbm, down_w),
                (mixer_hbm, mixer_w),
            ]
        )
    ]
    for load in loads:
        load.start()

    barrier = pltpu.get_barrier_semaphore()

    def greet(j, carry):
        pl.semaphore_signal(
            barrier, inc=1, device_id={"ep": (e + j) % n}, device_id_type=pl.DeviceIdType.MESH
        )
        return carry

    lax.fori_loop(1, n, greet, 0)
    for p in range(1, T):
        pl.semaphore_signal(
            barrier, inc=1, device_id={"tp": (t + p) % T}, device_id_type=pl.DeviceIdType.MESH
        )

    low = jnp.minimum(z, nz - 1 - z)
    left = z * 2 < nz

    inner = low > 0

    def line(k):
        outward = ((k + 1) // 2) * (2 * (k % 2) - 1)
        around = jnp.where(left, z - outward, z + outward)
        return jnp.where(k <= 2 * low, around, jnp.where(left, k, nz - 1 - k))

    def chip(k):
        if nz != 4:
            return line(k)
        near = jnp.where(k == 2, 3, jnp.where(k == 3, 2, k))
        return line(jnp.where(inner, near, jnp.where(k == 0, 0, k % 3 + 1)))

    def rdma(src, dst, ss, rs, axis, index):
        return pltpu.make_async_remote_copy(
            src_ref=src,
            dst_ref=dst,
            send_sem=ss,
            recv_sem=rs,
            device_id={axis: index},
            device_id_type=pl.DeviceIdType.MESH,
        )

    class Swap:
        def __init__(self, view, send, recv, k):
            self.view, self.send, self.recv, self.k = view, send, recv, k

        def copy(self, slot, owner, half, peer):
            block = self.view(owner, half)
            return rdma(
                block, block, self.send.at[slot, self.k], self.recv.at[slot, self.k], "tp", peer
            )

        def plan(self):
            x_next, y_next = t + 1 - 2 * (t % 2), (t + 2) % 4
            return [
                (0, t, None, x_next),
                (1, t, None, y_next),
                (2, x_next, 0, y_next),
                (3, y_next, 1, x_next),
            ]

        def start(self):
            if T == 4:
                for slot, owner, half, peer in self.plan()[:2]:
                    self.copy(slot, owner, half, peer).start()
            else:
                for p in range(1, T):
                    self.copy(p - 1, t, None, (t + p) % T).start()

        def relay(self):
            if T == 4:
                x_next, y_next = t + 1 - 2 * (t % 2), (t + 2) % 4
                for first, owner, plan in (
                    (0, x_next, self.plan()[2]),
                    (1, y_next, self.plan()[3]),
                ):
                    self.copy(first, owner, None, owner).wait_recv()
                    self.copy(*plan).start()

        def finish(self):
            if T == 4:
                for slot in (2, 3):
                    self.copy(slot, 3 - t, slot - 2, 3 - t).wait_recv()
            else:
                for p in range(1, T):
                    owner = (t + T - p) % T
                    self.copy(p - 1, owner, None, owner).wait_recv()

        def drain(self):
            if T == 4:
                for slot, owner, half, peer in self.plan():
                    self.copy(slot, owner, half, peer).wait_send()
            else:
                for p in range(1, T):
                    self.copy(p - 1, t, None, (t + p) % T).wait_send()

    def pair_at(k):
        return pl.ds(chip(k) * CORES, CORES)

    def pair_view(buffer, k):
        def view(owner, half):
            if half is None:
                return buffer.at[owner, pair_at(k)]
            return buffer.at[owner, chip(k) * CORES + half]

        return view

    def g_swap(k):
        return Swap(pair_view(incoming, k), g_send, g_recv, k)

    def h_swap(k):
        return Swap(pair_view(hid, k), h_send, h_recv, k)

    def a_swap(part):
        def view(owner, half):
            if half is None:
                return att_all.at[owner, part]
            return att_all.at[owner, part, pl.ds(half * (rows // 2), rows // 2)]

        return Swap(view, a_send, a_recv, part)

    def d_copy(dest, origin):
        return rdma(
            disp.at[dest], incoming.at[t, origin], d_send.at[dest], d_recv.at[origin], "ep", dest
        )

    near_copy = rdma(near, incoming.at[:, e], near_sem.at[0], near_sem.at[1], "ep", sibling)
    near_in = rdma(near, incoming.at[:, sibling], near_sem.at[0], near_sem.at[1], "ep", sibling)

    def kv_copies(zk, core, send, recv, dest):
        at = pl.ds(pl.multiple_of(core * rows, rows), rows)
        keys = k_all.at[zk, at]
        values = v_all.at[zk, :, 0:head_width, at]
        return [
            rdma(keys, keys, send.at[0, zk], recv.at[0, zk], "ep", dest),
            rdma(values, values, send.at[1, zk], recv.at[1, zk], "ep", dest),
        ]

    def kv_step(zk, direction):
        send = kv_up if direction > 0 else kv_down
        return kv_copies(zk, c, send, kv_recv, (e + direction * CORES + n) % n)

    def kv_across(zk):
        return kv_copies(zk, c, f_send, f_recv, sibling)

    def kv_pass(zk, act):
        @pl.when((zk <= z) & (z + 1 < nz))
        def _():
            for copy in kv_step(zk, 1):
                act(copy)

        @pl.when((zk >= z) & (z > 0))
        def _():
            for copy in kv_step(zk, -1):
                act(copy)

        for copy in kv_across(zk):
            act(copy)

    def places():
        expert = lax.broadcasted_iota(jnp.int32, (n, token_count), 0)
        named = [expert == rows_ref[k : k + 1, :] for k in range(top)]
        count = sum(jnp.where(x, 1.0, 0.0) for x in named).astype(bf)
        i = lax.broadcasted_iota(jnp.int32, (token_count, token_count), 0)
        j = lax.broadcasted_iota(jnp.int32, (token_count, token_count), 1)
        earlier = jnp.dot(
            count, jnp.where(i < j, 1.0, 0.0).astype(bf), preferred_element_type=f32
        )
        by_row = [
            rows_ref[k : k + 1, :].astype(f32) * capp
            + jnp.sum(jnp.where(named[k], earlier, 0.0), axis=0, keepdims=True)
            for k in range(top)
        ]
        width = 128
        weights = [weight_ref[k : k + 1, :] for k in range(top)]
        total = sum(weights)
        lines = by_row + [x / total for x in weights]
        lines.append(jnp.zeros((width - len(lines), token_count), f32))
        by_col = jnp.concatenate(lines, axis=0).T
        return by_row, by_col

    table_width = cos_table.shape[1]
    grid_rows = rows // GRID_W
    lane = lax.broadcasted_iota(jnp.int32, (GRID_W, table_width), 1)
    by_grid_row = (lane // (head_width // 4)) % 2 == 0
    for table, out in ((cos_table, cos_ref), (sin_table, sin_ref)):
        for r in range(grid_rows):
            out[r * GRID_W : (r + 1) * GRID_W] = jnp.where(
                by_grid_row, table[r : r + 1], table[grid_rows:]
            )

    def gain_rows(ref, width):
        gain = ref[...]
        flipped = [gain[:, head_width // 2 :], gain[:, : head_width // 2]]
        times = width // head_width
        return (
            jnp.concatenate([gain] * times, axis=1) if times > 1 else gain,
            jnp.concatenate(flipped * times, axis=1),
        )

    q_gain, q_gain_swapped = gain_rows(q_gain_ref, gw)
    k_gain, k_gain_swapped = gain_rows(k_gain_ref, pw)

    by_row, by_col = places()

    loads[0].wait()
    strip = math.gcd(token_count, 64)

    def normalise(i, carry):
        at = pl.ds(pl.multiple_of(i * strip, strip), strip)
        values = x_in[at].astype(f32)
        inv = lax.rsqrt(jnp.mean(values * values, axis=1, keepdims=True) + epsilon)
        normed[at] = (values * inv * moe_gain_ref[...]).astype(bf)
        return carry

    lax.fori_loop(0, token_count // strip, normalise, 0)

    def chosen(first, count):
        slot = lax.broadcasted_iota(jnp.int32, (count, token_count), 0).astype(f32)
        slot = slot + (first * capp).astype(f32)
        return sum(jnp.where(slot == place, 1.0, 0.0) for place in by_row).astype(bf)

    pl.semaphore_wait(barrier, n - 1 + T - 1)
    own_features = pl.ds(pl.multiple_of(t * feat, feat), feat)

    def make_disp(k, carry):
        part = jnp.dot(
            chosen(chip(k) * CORES, CORES * capp),
            normed[:, own_features],
            preferred_element_type=f32,
        ).astype(bf)
        disp[pair_at(k)] = part.reshape(CORES, capp, feat)
        return carry

    def send_disp(i, carry):
        k = jnp.where(i == 1, 1, nz + 1 - i)
        for cc in range(CORES):
            d_copy(line(k) * CORES + cc, e).start()
        return carry

    lax.fori_loop(1, nz, make_disp, 0)
    lax.fori_loop(1, nz, send_disp, 0)
    loads[1].wait()
    loads[2].wait()
    own_keys = pl.ds(pl.multiple_of(c * rows, rows), rows)
    for p in range(kw // pw):
        lanes = slice(p * pw, (p + 1) * pw)
        k_all[z, own_keys, lanes] = norm_rotate(
            k_in[:, lanes],
            k_gain,
            k_gain_swapped,
            cos_ref[:, :pw],
            sin_ref[:, :pw],
            head_width,
        )
        turned = v_in[:, lanes].astype(f32).T.astype(bf)
        for i in range(pw // head_width):
            v_all[z, p * (pw // head_width) + i, 0:head_width, own_keys] = turned[
                i * head_width : (i + 1) * head_width
            ]

    kv_pass(z, lambda copy: copy.start())

    own_pick = chosen(e, capp)
    sibling_pick = chosen(sibling, capp)
    for s in range(T):
        at = slice(s * feat, (s + 1) * feat)
        near[s] = jnp.dot(sibling_pick, normed[:, at], preferred_element_type=f32).astype(bf)
    near_copy.start()
    for s in range(T):
        at = slice(s * feat, (s + 1) * feat)
        incoming[s, e] = jnp.dot(own_pick, normed[:, at], preferred_element_type=f32).astype(bf)

    def spread(k):
        for cc in range(CORES):
            d_copy(chip(k) * CORES + cc, chip(k) * CORES + cc).wait_recv()
        g_swap(k).start()

    v_all[:, :, head_width:, :] = jnp.ones(
        (nz, kh, v_all.shape[2] - head_width, CORES * rows), bf
    )
    m_ref[...] = jnp.full(m_ref.shape, -jnp.inf, f32)
    acc_ref[...] = jnp.zeros(acc_ref.shape, f32)
    slots = lax.broadcasted_iota(jnp.int32, (token_count, n * capp), 1).astype(f32)
    for k in range(top):
        pick[k] = jnp.where(slots == by_col[:, k : k + 1], 1.0, 0.0).astype(bf)
        share_ref[k] = by_col[:, top + k : top + k + 1]

    loads[3].wait()
    for h in range(kh):
        turned = norm_rotate(
            q_in[:, h * gw : (h + 1) * gw],
            q_gain,
            q_gain_swapped,
            cos_ref[:, :gw],
            sin_ref[:, :gw],
            head_width,
        )
        place = (h * head_width) % pw
        for g in range(group):
            parts = [turned[:, g * head_width : (g + 1) * head_width]]
            if place:
                parts.insert(0, jnp.zeros((rows, place), bf))
            if pw - place - head_width:
                parts.append(jnp.zeros((rows, pw - place - head_width), bf))
            q_all[h, g * rows : (g + 1) * rows] = (
                jnp.concatenate(parts, axis=1) if len(parts) > 1 else parts[0]
            )

    factor = math.log2(math.e) * head_width ** (-0.5)
    step_rows = math.gcd(group_rows, 512)

    parts = att_all.shape[1]
    heads_part = kh // parts

    def attend(zk, first=0, last=kh):
        def one_head(h, carry):
            lanes = pl.ds(pl.multiple_of((h * head_width) // pw * pw, pw), pw)
            keys = k_all[zk, :, lanes] if kh > 1 else k_all[zk]
            values = v_all[zk, h]

            def scores_at(r):
                return lax.dot_general(
                    keys,
                    q_all[h, r : r + step_rows],
                    (((1,), (1,)), ((), ())),
                    preferred_element_type=f32,
                )

            later = scores_at(0)
            for r in range(0, group_rows, step_rows):
                scores = later
                if r + step_rows < group_rows:
                    later = scores_at(r + step_rows)
                at = slice(r, r + step_rows)
                old = m_ref[h, :, at]
                new = jnp.maximum(old, jnp.max(scores, axis=0, keepdims=True))
                weights = jnp.exp2(scores * factor - new * factor).astype(bf)
                m_ref[h, :, at] = new
                acc_ref[h, :, at] = acc_ref[h, :, at] * jnp.exp2((old - new) * factor) + jnp.dot(
                    values, weights, preferred_element_type=f32
                )
            return carry

        lax.fori_loop(first, last, one_head, 0)

    def kv_arrive(k):
        zk = line(k)

        @pl.when(zk != z)
        def _():
            for copy in kv_step(zk, 1):
                copy.wait_recv()
            kv_pass(zk, lambda copy: copy.start())

    def kv_join(k):
        for copy in kv_copies(line(k), 1 - c, f_send, f_recv, sibling):
            copy.wait_recv()

    def first_half(k):
        @pl.when(k == 0)
        def _():
            near_in.wait_recv()

        @pl.when(k > 0)
        def _():
            g_swap(k).finish()

        gate = jnp.zeros((CORES * capp, ffl), f32)
        up = jnp.zeros((CORES * capp, ffl), f32)
        for s in range(T):
            piece = incoming[s, pair_at(k)].reshape(CORES * capp, feat)
            at = slice(s * feat, (s + 1) * feat)
            gate = gate + jnp.dot(piece, gate_w[at], preferred_element_type=f32)
            up = up + jnp.dot(piece, up_w[at], preferred_element_type=f32)
        hidden = (gate / (1.0 + jnp.exp(-gate)) * up).astype(bf)
        hid[t, pair_at(k)] = hidden.reshape(CORES, capp, ffl)
        h_swap(k).start()

    def r_copy(dest, origin):
        return rdma(eo.at[dest], ret.at[origin], r_send.at[dest], r_recv.at[origin], "ep", dest)

    def second_half(k):
        h_swap(k).finish()
        total = jnp.zeros((CORES * capp, cols), f32)
        for s in range(T):
            piece = hid[s, pair_at(k)].reshape(CORES * capp, ffl)
            total = total + jnp.dot(
                piece, down_w[s * ffl : (s + 1) * ffl], preferred_element_type=f32
            )
        eo[pair_at(k)] = total.astype(bf).reshape(CORES, capp, cols)

    def send_back(k):
        for cc in range(CORES):
            origin = chip(k) * CORES + cc

            @pl.when(origin != e)
            def _():
                r_copy(origin, e).start()

            @pl.when(origin == e)
            def _():
                ret[origin] = eo[origin]

    def finish_heads(part):
        for i in range(heads_part):
            h = part * heads_part + i
            done = acc_ref[h, 0:head_width] / acc_ref[h, head_width : head_width + 1]
            done = jnp.concatenate(
                [done[:, g * rows : (g + 1) * rows] for g in range(group)], axis=0
            )
            att_all[t, part, :, i * gw : (i + 1) * gw] = done.T.astype(bf)
        a_swap(part).start()

    def tuned():
        outer = jnp.logical_not(inner)
        spread(1)
        kv_join(0)
        attend(z)
        for load in loads[4:7]:
            load.wait()
        first_half(0)
        g_swap(1).relay()
        spread(2)
        h_swap(0).relay()
        first_half(1)
        spread(3)
        g_swap(2).relay()
        second_half(0)
        send_back(0)
        h_swap(1).relay()
        kv_arrive(1)
        kv_join(1)
        attend(line(1), 0, kh // 2)

        @pl.when(inner)
        def _():
            kv_arrive(2)

        @pl.when(outer)
        def _():
            attend(line(1), kh // 2, kh)

        g_swap(3).relay()

        @pl.when(inner)
        def _():
            attend(line(1), kh // 2, kh)

        first_half(2)
        second_half(1)

        @pl.when(inner)
        def _():
            kv_arrive(3)
            send_back(1)

        h_swap(2).relay()
        first_half(3)

        @pl.when(outer)
        def _():
            send_back(1)

        second_half(2)

        @pl.when(outer)
        def _():
            kv_arrive(2)

        h_swap(3).relay()
        kv_join(2)
        attend(line(2), 0, kh // 2)
        second_half(3)
        send_back(3)
        attend(line(2), kh // 2, kh)
        send_back(2)

        @pl.when(outer)
        def _():
            kv_arrive(3)

        kv_join(3)
        for part in range(parts):
            attend(line(3), part * heads_part, (part + 1) * heads_part)
            finish_heads(part)

    def general():
        kv_join(0)
        attend(z)
        for load in loads[4:7]:
            load.wait()
        if nz > 1:
            spread(1)

        def step(j, carry):
            @pl.when(j < nz)
            def _():
                first_half(j)

            @pl.when(j + 1 < nz)
            def _():
                g_swap(j + 1).relay()

            @pl.when(j + 2 < nz)
            def _():
                spread(j + 2)

            @pl.when((j >= 1) & (j < nz))
            def _():
                kv_arrive(j)

            @pl.when(j >= 1)
            def _():
                h_swap(j - 1).relay()

            @pl.when(j >= 2)
            def _():
                kv_join(j - 1)
                attend(line(j - 1))

            @pl.when(j >= 1)
            def _():
                second_half(j - 1)
                send_back(j - 1)

            return carry

        lax.fori_loop(0, nz + 1, step, 0)
        for part in range(parts):
            finish_heads(part)

    if nz == 4:
        tuned()
    else:
        general()

    loads[7].wait()
    aw = parts * att_all.shape[3]
    out_cols = attn_ref.shape[1]
    half = math.gcd(out_cols, 256)

    def strip_out(i):
        at = pl.ds(pl.multiple_of(i * half, half), half)
        return pltpu.make_async_copy(attn_ref.at[:, at], attn_hbm.at[:, at], o_sem.at[i + 1])

    moe_out = pltpu.make_async_copy(moe_ref, moe_hbm, o_sem.at[0])

    def mix(owners, opening, closing):
        def strip_of(i, carry):
            at = pl.ds(pl.multiple_of(i * half, half), half)
            total = jnp.zeros((rows, half), f32) if opening else mix_acc[:, at]
            for s in owners:
                for part in range(parts):
                    width = aw // parts
                    lines = pl.ds(pl.multiple_of(s * aw + part * width, width), width)
                    total = total + jnp.dot(
                        att_all[s, part], mixer_w[lines, at], preferred_element_type=f32
                    )
            if closing:
                attn_ref[:, at] = total.astype(bf)
                strip_out(i).start()
            else:
                mix_acc[:, at] = total
            return carry

        lax.fori_loop(0, out_cols // half, strip_of, 0)

    def gather_experts():
        def wait_ret(j, carry):
            origin = (e + j) % n
            r_copy(origin, origin).wait_recv()
            return carry

        lax.fori_loop(1, n, wait_ret, 0)
        returned = ret[...].reshape(n * capp, cols)
        combined = jnp.zeros(moe_ref.shape, f32)
        for k in range(top):
            combined = combined + share_ref[k] * jnp.dot(
                pick[k], returned, preferred_element_type=f32
            )
        moe_ref[...] = combined.astype(bf)
        moe_out.start()

    mix([t], True, False)
    for part in range(parts):
        a_swap(part).relay()
    if T == 4:
        mix([t + 1 - 2 * (t % 2), (t + 2) % 4], False, False)
    gather_experts()
    for part in range(parts):
        a_swap(part).finish()
    if T == 4:
        mix([3 - t], False, True)
    else:
        mix([(t + p) % T for p in range(1, T)], False, True)

    near_copy.wait_send()

    def drain_ep(j, carry):
        r_copy((e + j) % n, e).wait_send()
        return carry

    lax.fori_loop(1, n, drain_ep, 0)

    def drain(k, carry):
        kv_pass(k, lambda copy: copy.wait_send())
        h_swap(k).drain()

        @pl.when(k > 0)
        def _():
            g_swap(k).drain()
            for cc in range(CORES):
                d_copy(chip(k) * CORES + cc, e).wait_send()

        return carry

    lax.fori_loop(0, nz, drain, 0)
    for part in range(parts):
        a_swap(part).drain()
    moe_out.wait()

    def drain_out(i, carry):
        strip_out(i).wait()
        return carry

    lax.fori_loop(0, out_cols // half, drain_out, 0)


def hand_over(attn_in, moe_in, attn_out, moe_out, attn_buf, moe_buf, in_sem, out_sem):
    pieces = []
    for src, buf, dst in ((attn_in, attn_buf, attn_out), (moe_in, moe_buf, moe_out)):
        size = math.gcd(src.shape[0], 128)
        for r in range(0, src.shape[0], size):
            at = pl.ds(r, size)
            i = len(pieces)
            pieces.append(
                (
                    pltpu.make_async_copy(src.at[at], buf.at[at], in_sem.at[i]),
                    pltpu.make_async_copy(buf.at[at], dst.at[at], out_sem.at[i]),
                )
            )
    for read, _ in pieces:
        read.start()
    for read, write in pieces:
        read.wait()
        write.start()
    for _, write in pieces:
        write.wait()


def on_device(
    n,
    T,
    query_input,
    key_input,
    value_input,
    query_gain,
    key_gain,
    mixer_out,
    moe_input,
    moe_gain,
    routes,
    route_weight,
    expert_gate,
    expert_up,
    expert_down,
):
    rows = query_input.shape[0]
    head_width = query_gain.shape[0]
    heads_here = query_input.shape[1] // head_width
    kw = key_input.shape[1]
    kh = kw // head_width
    group = heads_here // kh
    pw = min(128, kw)
    gw = group * head_width
    width = max(gw, pw)
    assert rows % GRID_W == 0
    grid_rows = rows // GRID_W
    cosine, sine = rope_tables(lax.axis_index("ep") * grid_rows, grid_rows, head_width, width)

    token_count, model_width = moe_input.shape
    top = routes.shape[1]
    local_experts = expert_gate.shape[0]
    assert local_experts == 1
    expert_count = local_experts * n
    capacity = 3 * token_count * top // (2 * expert_count)
    capp = -(-capacity // 16) * 16
    feat = model_width // T
    gate = expert_gate[0]
    up = expert_up[0]
    down = expert_down[0]
    ffl = gate.shape[1]
    cols = down.shape[1]
    nz = n // CORES
    aw = heads_here * head_width
    out_cols = mixer_out.shape[1]
    slots = 4 if T == 4 else T - 1
    parts = kh
    bf = jnp.bfloat16
    dma = pltpu.SemaphoreType.DMA
    vmem = pl.BlockSpec(memory_space=pltpu.VMEM)
    hbm = pl.BlockSpec(memory_space=pl.ANY)
    attn, moe = pl.pallas_call(
        functools.partial(kernel, (n, T, head_width)),
        out_shape=(
            jax.ShapeDtypeStruct((rows, out_cols), bf),
            jax.ShapeDtypeStruct((token_count, cols), bf),
        ),
        in_specs=[hbm] * 8 + [vmem] * 7,
        out_specs=(hbm, hbm),
        scratch_shapes=[
            pltpu.VMEM((rows, out_cols), bf),
            pltpu.VMEM((token_count, cols), bf),
            dma((1 + out_cols // math.gcd(out_cols, 256),)),
            pltpu.VMEM(moe_input.shape, bf),
            pltpu.VMEM(query_input.shape, bf),
            pltpu.VMEM(key_input.shape, bf),
            pltpu.VMEM(value_input.shape, bf),
            pltpu.VMEM(moe_input.shape, bf),
            pltpu.VMEM((n, capp, feat), bf),
            pltpu.VMEM((T, capp, feat), bf),
            pltpu.VMEM((top, token_count, n * capp), bf),
            pltpu.VMEM((top, token_count, 1), jnp.float32),
            pltpu.VMEM((rows, width), jnp.float32),
            pltpu.VMEM((rows, width), jnp.float32),
            pltpu.VMEM((kh, group * rows, pw), bf),
            pltpu.VMEM((nz, CORES * rows, kw), bf),
            pltpu.VMEM((nz, kh, head_width + ONES, CORES * rows), bf),
            pltpu.VMEM((T, n, capp, feat), bf),
            pltpu.VMEM((T, n, capp, ffl), bf),
            pltpu.VMEM((n, capp, cols), bf),
            pltpu.VMEM((n, capp, cols), bf),
            pltpu.VMEM((T, parts, rows, aw // parts), bf),
            pltpu.VMEM((rows, out_cols), jnp.float32),
            pltpu.VMEM(gate.shape, bf),
            pltpu.VMEM(up.shape, bf),
            pltpu.VMEM(down.shape, bf),
            pltpu.VMEM(mixer_out.shape, bf),
            pltpu.VMEM((kh, 1, group * rows), jnp.float32),
            pltpu.VMEM((kh, head_width + ONES, group * rows), jnp.float32),
            dma((8,)),
            dma((n,)),
            dma((n,)),
            dma((2,)),
            dma((2, nz)),
            dma((2, nz)),
            dma((2, nz)),
            dma((2, nz)),
            dma((2, nz)),
            dma((slots, nz)),
            dma((slots, nz)),
            dma((slots, nz)),
            dma((slots, nz)),
            dma((n,)),
            dma((n,)),
            dma((slots, parts)),
            dma((slots, parts)),
        ],
        compiler_params=pltpu.CompilerParams(
            collective_id=0, has_side_effects=True, vmem_limit_bytes=63 * 1024 * 1024
        ),
    )(
        moe_input,
        query_input,
        key_input,
        value_input,
        gate,
        up,
        down,
        mixer_out,
        cosine,
        sine,
        query_gain[None, :],
        key_gain[None, :],
        moe_gain[None, :],
        routes.T,
        route_weight.T,
    )
    count = rows // math.gcd(rows, 128) + token_count // math.gcd(token_count, 128)
    return pl.pallas_call(
        hand_over,
        out_shape=(
            jax.ShapeDtypeStruct(attn.shape, bf),
            jax.ShapeDtypeStruct(moe.shape, bf),
        ),
        in_specs=[hbm] * 2,
        out_specs=(hbm, hbm),
        scratch_shapes=[
            pltpu.VMEM(attn.shape, bf),
            pltpu.VMEM(moe.shape, bf),
            dma((count,)),
            dma((count,)),
        ],
        compiler_params=pltpu.CompilerParams(vmem_limit_bytes=63 * 1024 * 1024),
    )(attn, moe)


def solution(mesh):
    placed = (
        P("ep", "tp"),
        P("ep", "tp"),
        P("ep", "tp"),
        P(),
        P(),
        P(None, "tp"),
        P("ep", None),
        P(),
        P("ep", None),
        P("ep", None),
        P("ep", None, "tp"),
        P("ep", None, "tp"),
        P("ep", None, "tp"),
    )
    return jax.shard_map(
        functools.partial(on_device, mesh.shape["ep"], mesh.shape["tp"]),
        mesh=mesh,
        in_specs=placed,
        out_specs=(P("ep", "tp"), P("ep", "tp")),
        check_vma=False,
    )
```
